32 devices in a mesh: ep: 8 (over z, core), tp: 4 (over y, x).
Axes of the slice: x: 2, y: 2, z: 4, core: 2. Of those that a mesh axis runs over, the one named last changes fastest.
Arguments:
- tokens: bfloat16 [1024, 2048], P('ep'), may hold values from -6 to 6
- chosen: int32 [8, 8, 8], replicated, may hold values from 0 to 127, as said below
- chosen_weight: float32 [8, 8, 8], P('ep'), may hold values from 0.1 to 1
- gate_weight: bfloat16 [8, 2048, 4096], P('ep', None, 'tp'), may hold values from -0.125 to 0.125
- up_weight: bfloat16 [8, 2048, 4096], P('ep', None, 'tp'), may hold values from -0.125 to 0.125
- down_weight: bfloat16 [8, 4096, 2048], P('ep', 'tp'), may hold values from -0.09375 to 0.09375
Outputs:
- combined: bfloat16 [1024, 2048], P('ep', 'tp')
The draws below stay inside these ranges and needn't reach their ends.
Inputs may be any that keep to these rules, and one draw needn't show every extreme that they name: `chosen`: for every block and expert the 8 positions are distinct.
All inputs are finite; a program needn't handle non-finite values.
Results may differ from the reference program's by a relative error of at most 0.015.
Values may be sent and summed in bfloat16 or wider, within the bound.
A program may use at most 64 MiB of HBM per device.

```python
import jax
import jax.numpy as jnp
from jax import lax

D = 2048
FF = 4096
TOK_DEV = 128
PICK = 8
BLOCKS = 8
EXPERTS = 8
TOKENS = 1024
N_TP = 4


def draw_chosen(key, part):
    keys = jax.random.split(jax.random.fold_in(key, 11), BLOCKS * EXPERTS)
    orders = jax.vmap(lambda single: jax.random.permutation(single, TOK_DEV)[:PICK])(keys)
    return orders.reshape(BLOCKS, EXPERTS, PICK).astype(jnp.int32)


def shard_levels(stream_key, dims, cuts, low, top_value):
    def one(dim, blocks):
        draws = jax.random.uniform(jax.random.fold_in(jax.random.fold_in(stream_key, 6), dim), (blocks,), jnp.float32, low / len(cuts), top_value / len(cuts))
        return jnp.repeat(jnp.exp(draws), dims[dim] // blocks).reshape((-1,) + (1,) * (len(dims) - dim - 1))

    gain = one(*cuts[0])
    for cut in cuts[1:]:
        gain = gain * one(*cut)
    return gain


def gaussian(own_key, extent, width, most, cuts=(), kind=jnp.bfloat16):
    loudness = shard_levels(own_key, extent, cuts, -0.22, 0.18) if cuts else 1.0
    values = jax.random.normal(own_key, extent, jnp.float32) * width * loudness
    return jnp.minimum(jnp.maximum(values, -most), most).astype(kind)


def setup_inputs(seed: int = 0) -> dict:
    splits = jax.random.split(jax.random.key(seed), 7)
    tokens = gaussian(splits[0], (TOKENS, D), 1.0, 6.0, ((0, 8),))
    chosen = draw_chosen(jax.random.fold_in(splits[6], 71), 0)
    chosen_weight = jnp.clip(0.1 + 0.9 * jax.random.uniform(splits[2], (BLOCKS, EXPERTS, PICK), jnp.float32) ** shard_levels(splits[2], (BLOCKS, EXPERTS, PICK), ((0, 8),), -0.2, 0.2), 0.1, 1.0)
    gate_weight = gaussian(splits[3], (EXPERTS, D, FF), D ** -0.5, 0.125, ((0, 8), (2, 4)))
    up_weight = gaussian(splits[4], (EXPERTS, D, FF), D ** -0.5, 0.125, ((0, 8), (2, 4)))
    down_weight = gaussian(splits[5], (EXPERTS, FF, D), FF ** -0.5, 0.09375, ((0, 8), (1, 4)))
    return {"tokens": tokens, "chosen": chosen, "chosen_weight": chosen_weight, "gate_weight": gate_weight, "up_weight": up_weight, "down_weight": down_weight}


def reference(tokens, chosen, chosen_weight, gate_weight, up_weight, down_weight):
    offsets = (jnp.arange(BLOCKS, dtype=jnp.int32) * TOK_DEV)[:, None, None]
    global_rows = (chosen + offsets).astype(jnp.int32)
    per_expert = jnp.transpose(global_rows, (1, 0, 2)).reshape(EXPERTS, BLOCKS * PICK)
    slice_width = FF // N_TP

    def expert_pass(inputs):
        picked, gate_local, up_local, down_local = inputs
        selected = jnp.take(tokens, picked, axis=0)
        gate_sum = jnp.dot(selected, gate_local, preferred_element_type=jnp.float32)
        up_sum = jnp.dot(selected, up_local, preferred_element_type=jnp.float32)
        hidden = (jax.nn.silu(gate_sum) * up_sum).astype(jnp.bfloat16)
        partials = jnp.einsum("rtf,tfd->trd",
                              hidden.reshape(-1, N_TP, slice_width).astype(jnp.float32),
                              down_local.reshape(N_TP, slice_width, D).astype(jnp.float32))
        rounded = lax.optimization_barrier(partials.astype(jnp.bfloat16))
        return jnp.sum(rounded.astype(jnp.float32), axis=0).astype(jnp.bfloat16)

    outputs = lax.map(expert_pass, (per_expert, gate_weight, up_weight, down_weight))
    arranged = jnp.transpose(outputs.reshape(EXPERTS, BLOCKS, PICK, D), (1, 0, 2, 3))
    weighted = arranged.astype(jnp.float32) * chosen_weight[..., None]
    combined = jnp.zeros((BLOCKS * TOK_DEV, D), jnp.float32).at[global_rows.reshape(-1)].add(weighted.reshape(-1, D))
    return combined.astype(jnp.bfloat16)
```

```python
import functools

import jax
import jax.numpy as jnp
from jax import lax
from jax.experimental import pallas as pl
from jax.experimental.pallas import tpu as pltpu
from jax.sharding import PartitionSpec as P

MESH = pl.DeviceIdType.MESH
GROUPS = 4
EARLY = 2


def each(count, body):
    if count <= 8:
        for i in range(count):
            body(i)
    else:
        pl.loop(0, count)(body)


def kernel(
    n_ep, n_tp,
    tok_hbm, cho_hbm, wt_hbm, gate_hbm, up_hbm, down_hbm,
    out_ref,
    tok, cho, wt, gate, up, down,
    leaving, arrived, gate_acc, up_acc, place,
    part_out, part_in, back_out, back_in,
    in_sem, w_sem, d_sem,
    s1_send, s1_recv, hop_send, hop_recv, fan_send, fan_recv, s2_send, s2_recv, s3_send, s3_recv,
    ep_ready, tp_ready,
):
    e = lax.axis_index("ep")
    t = lax.axis_index("tp")
    tok_count, width = tok.shape
    experts, picks = cho.shape
    rows = experts * picks
    sw = width // n_tp
    gs = n_ep // GROUPS
    mine = e // gs

    def group_at(i):
        if i == GROUPS - 1:
            return mine
        low = GROUPS - 1 - i
        low = jnp.where(low > mine, low, low - 1)
        high = jnp.where(i < mine, i, i + 1)
        return jnp.where(mine < GROUPS // 2, low, high)

    def quarter_at(i):
        if i == n_tp - 1:
            return t
        down_first = n_tp - 1 - i
        up_first = jnp.where(i < t, i, i + 1)
        return jnp.where(t == 0, down_first, up_first)

    barrier = pltpu.get_barrier_semaphore()

    def greet(p):
        pl.semaphore_signal(barrier, inc=1, device_id={"ep": p}, device_id_type=MESH)

    pl.loop(e + 1, n_ep)(greet)

    def greet_tp(p):
        pl.semaphore_signal(barrier, inc=1, device_id={"tp": p}, device_id_type=MESH)

    pl.loop(t + 1, n_tp)(greet_tp)

    loads = [
        pltpu.make_async_copy(cho_hbm.at[e], cho, in_sem.at[0]),
        pltpu.make_async_copy(wt_hbm.at[0], wt, in_sem.at[1]),
        pltpu.make_async_copy(tok_hbm, tok, in_sem.at[2]),
    ]
    for c in loads:
        c.start()
    wloads = []
    for k in range(n_tp):
        piece = pl.ds(k * sw, sw)
        a = pltpu.make_async_copy(gate_hbm.at[0, piece, :], gate.at[piece, :], w_sem.at[0, k])
        b = pltpu.make_async_copy(up_hbm.at[0, piece, :], up.at[piece, :], w_sem.at[1, k])
        wloads.append((a, b))
    dloads = []
    for i in range(n_tp):
        col = pl.multiple_of(quarter_at(i) * sw, sw)
        dloads.append(
            pltpu.make_async_copy(down_hbm.at[0, :, pl.ds(col, sw)], down.at[i], d_sem.at[i])
        )

    with jax.named_scope("barrier"):
        @pl.when(e + t > 0)
        def _():
            pl.semaphore_wait(barrier, e + t)

    def answer(p):
        pl.semaphore_signal(ep_ready.at[e], inc=1, device_id={"ep": p}, device_id_type=MESH)

    pl.loop(0, e)(answer)

    def answer_tp(p):
        pl.semaphore_signal(tp_ready, inc=1, device_id={"tp": p}, device_id_type=MESH)

    pl.loop(0, t)(answer_tp)

    with jax.named_scope("loadwait"):
        for c in loads:
            c.wait()
    for a, b in wloads:
        a.start()
        b.start()
    for c in dloads:
        c.start()

    lane = lax.broadcasted_iota(jnp.int32, (picks, picks), 1)
    sub = lax.broadcasted_iota(jnp.int32, (picks, picks), 0)
    diag = lane == sub
    position = lax.broadcasted_iota(jnp.int32, (picks, tok_count), 1).astype(jnp.float32)
    columns, hots = [], []
    for x in range(experts):
        spread = jnp.broadcast_to(cho[x : x + 1, :], (picks, picks)).astype(jnp.float32)
        column = jnp.sum(jnp.where(diag, spread, 0.0), axis=1, keepdims=True)
        columns.append(column)
        hots.append(jnp.where(position == column, 1.0, 0.0))
    onehot = jnp.concatenate(hots, axis=0).astype(jnp.bfloat16)
    with jax.named_scope("gather"):
        for k in range(n_tp):
            sel = jnp.dot(
                onehot, tok[:, k * sw : (k + 1) * sw], preferred_element_type=jnp.float32
            )
            leaving[k] = sel.reshape(experts, picks, sw).astype(jnp.bfloat16)

    def send_tokens(k, p):
        return pltpu.make_async_remote_copy(
            src_ref=leaving.at[k, p],
            dst_ref=arrived.at[k, e],
            send_sem=s1_send,
            recv_sem=s1_recv.at[k],
            device_id={"ep": p},
            device_id_type=MESH,
        )

    def send_hop(p):
        return pltpu.make_async_remote_copy(
            src_ref=leaving.at[t, p],
            dst_ref=arrived.at[t, e],
            send_sem=hop_send,
            recv_sem=hop_recv,
            device_id={"ep": p},
            device_id_type=MESH,
        )

    def send_group(g):
        for k in range(n_tp):
            each(gs, lambda i: send_tokens(k, g * gs + i).start())

    def ready_group(g):
        each(gs, lambda i: pl.semaphore_wait(ep_ready.at[g * gs + i], 1))

    with jax.named_scope("senddown"):
        pl.loop(0, mine)(send_group)

        def send_near(i):
            p = mine * gs + i

            @pl.when(p > e)
            def _():
                pl.semaphore_wait(ep_ready.at[p], 1)

            @pl.when(p != e)
            def _():
                for k in range(n_tp):
                    send_tokens(k, p).start()

        each(gs, send_near)
    with jax.named_scope("sendup"):
        @pl.when(mine < GROUPS - 1)
        def _():
            ready_group(mine + 1)
            each(gs, lambda i: send_hop((mine + 1) * gs + i).start())

        def send_up(g):
            ready_group(g)
            send_group(g)

        pl.loop(mine + 2, GROUPS)(send_up)

    parts = []
    for x in range(experts):
        wide = jnp.broadcast_to(wt[x : x + 1, :], (picks, picks))
        wcol = jnp.sum(jnp.where(diag, wide, 0.0), axis=1, keepdims=True)
        parts.append(jnp.where(position == columns[x], wcol, 0.0))
    weighted = jnp.concatenate(parts, axis=0)
    hi = weighted.astype(jnp.bfloat16).astype(jnp.float32)
    mid = (weighted - hi).astype(jnp.bfloat16).astype(jnp.float32)
    lo = weighted - hi - mid
    place[...] = jnp.concatenate([hi, mid, lo], axis=0).T.astype(jnp.bfloat16)

    def landed(ref, sem):
        pltpu.make_async_copy(ref, ref, sem).wait()


    @pl.when(t < n_tp - 1)
    def _():
        pl.semaphore_wait(tp_ready, n_tp - 1 - t)

    below = pl.ds((mine - 1) * gs, gs)

    def send_fan(i):
        return pltpu.make_async_remote_copy(
            src_ref=arrived.at[t, below],
            dst_ref=arrived.at[t, below],
            send_sem=fan_send,
            recv_sem=fan_recv.at[t],
            device_id={"tp": quarter_at(i)},
            device_id_type=MESH,
        )

    with jax.named_scope("fan"):
        @pl.when(mine > 0)
        def _():
            landed(arrived.at[t, pl.ds(0, gs)], hop_recv)
            for i in range(n_tp - 1):
                send_fan(i).start()

    for k in range(n_tp):
        arrived[k, e] = leaving[k, e]

        with jax.named_scope(f'tokin#k={k}'):
            @pl.when(mine == 0)
            def _():
                landed(arrived.at[k, pl.ds(0, n_ep - 1)], s1_recv.at[k])

            @pl.when(mine > 0)
            def _():
                landed(arrived.at[k, pl.ds(0, n_ep - 1 - gs)], s1_recv.at[k])

            @pl.when(jnp.logical_and(mine > 0, t != k))
            def _():
                landed(arrived.at[k, pl.ds(0, gs)], fan_recv.at[k])

        x = arrived[k].astype(jnp.float32).reshape(rows, sw).astype(jnp.bfloat16)
        for c in wloads[k]:
            c.wait()
        g = jnp.dot(x, gate[k * sw : (k + 1) * sw, :], preferred_element_type=jnp.float32)
        u = jnp.dot(x, up[k * sw : (k + 1) * sw, :], preferred_element_type=jnp.float32)
        if k == 0:
            gate_acc[...] = g
            up_acc[...] = u
        elif k < n_tp - 1:
            gate_acc[...] += g
            up_acc[...] += u
    g = gate_acc[...] + g
    u = up_acc[...] + u
    with jax.named_scope("hidden"):
        hidden = (g / (1.0 + jnp.exp(-g)) * u).astype(jnp.bfloat16)

    def send_part(i, gi):
        blocks = pl.ds(group_at(gi) * gs, gs)
        return pltpu.make_async_remote_copy(
            src_ref=part_out.at[i, blocks],
            dst_ref=part_in.at[t, blocks],
            send_sem=s2_send,
            recv_sem=s2_recv.at[gi],
            device_id={"tp": quarter_at(i)},
            device_id_type=MESH,
        )

    def send_back(p):
        return pltpu.make_async_remote_copy(
            src_ref=back_out.at[p],
            dst_ref=back_in.at[e],
            send_sem=s3_send,
            recv_sem=s3_recv,
            device_id={"ep": p},
            device_id_type=MESH,
        )

    for i in range(n_tp):
        dloads[i].wait()
        with jax.named_scope(f'down#i={i}'):
            part = jnp.dot(hidden, down[i], preferred_element_type=jnp.float32)
            part_out[i] = part.reshape(experts, picks, sw).astype(jnp.bfloat16)
        if i < n_tp - 1:
            for gi in range(EARLY):
                send_part(i, gi).start()
        if i == n_tp - 2:
            for gi in range(EARLY, GROUPS):
                for x in range(n_tp - 1):
                    send_part(x, gi).start()
    for gi in range(GROUPS):
        gg = group_at(gi)
        total = part_out[n_tp - 1, pl.ds(gg * gs, gs)].astype(jnp.float32)
        with jax.named_scope(f'rs#g={gi}'):
            landed(part_in.at[pl.ds(0, n_tp - 1), pl.ds(gg * gs, gs)], s2_recv.at[gi])
        for i in range(n_tp - 1):
            total += part_in[quarter_at(i), pl.ds(gg * gs, gs)].astype(jnp.float32)
        back_out[pl.ds(gg * gs, gs)] = total.astype(jnp.bfloat16)

        def give(i):
            p = gg * gs + i
            if gi < GROUPS - 1:
                send_back(p).start()
            else:
                @pl.when(p != e)
                def _():
                    send_back(p).start()

        each(gs, give)
    back_in[e] = back_out[e]

    with jax.named_scope('backin'):
        landed(back_in.at[pl.ds(0, n_ep - 1)], s3_recv)
    with jax.named_scope("combine"):
        y = back_in[...].astype(jnp.float32).reshape(rows, sw).astype(jnp.bfloat16)
        y = jnp.concatenate([y, y, y], axis=0)
        result = jnp.dot(place[...], y, preferred_element_type=jnp.float32)
        out_ref[...] = result.astype(out_ref.dtype)

    with jax.named_scope("drain"):
        for k in range(n_tp):
            @pl.when(mine == GROUPS - 1)
            def _():
                landed(leaving.at[k, pl.ds(0, n_ep - 1)], s1_send)

            @pl.when(mine < GROUPS - 1)
            def _():
                landed(leaving.at[k, pl.ds(0, n_ep - 1 - gs)], s1_send)

        @pl.when(mine < GROUPS - 1)
        def _():
            landed(leaving.at[0, pl.ds(0, gs)], hop_send)

        @pl.when(mine > 0)
        def _():
            landed(arrived.at[pl.ds(0, n_tp - 1), pl.ds(0, gs)], fan_send)

        landed(part_out.at[pl.ds(0, n_tp - 1)], s2_send)
        landed(back_out.at[pl.ds(0, n_ep - 1)], s3_send)


def local(tokens, chosen, chosen_weight, gate_weight, up_weight, down_weight):
    n_ep, n_tp = lax.axis_size("ep"), lax.axis_size("tp")
    tok_count, width = tokens.shape
    blocks, experts, picks = chosen.shape
    hid = gate_weight.shape[2]
    rows = blocks * picks
    sw = width // n_tp
    bf, f32 = jnp.bfloat16, jnp.float32
    dma = pltpu.SemaphoreType.DMA
    hbm = pl.BlockSpec(memory_space=pltpu.HBM)
    return pl.pallas_call(
        functools.partial(kernel, n_ep, n_tp),
        out_shape=jax.ShapeDtypeStruct((tok_count, sw), bf),
        in_specs=[hbm] * 6,
        out_specs=pl.BlockSpec(memory_space=pltpu.VMEM),
        scratch_shapes=[
            pltpu.VMEM((tok_count, width), bf),
            pltpu.VMEM((experts, picks), jnp.int32),
            pltpu.VMEM((experts, picks), f32),
            pltpu.VMEM((width, hid), bf),
            pltpu.VMEM((width, hid), bf),
            pltpu.VMEM((n_tp, hid, sw), bf),
            pltpu.VMEM((n_tp, experts, picks, sw), bf),
            pltpu.VMEM((n_tp, blocks, picks, sw), bf),
            pltpu.VMEM((rows, hid), f32),
            pltpu.VMEM((rows, hid), f32),
            pltpu.VMEM((tok_count, 3 * experts * picks), bf),
            pltpu.VMEM((n_tp, blocks, picks, sw), bf),
            pltpu.VMEM((n_tp, blocks, picks, sw), bf),
            pltpu.VMEM((blocks, picks, sw), bf),
            pltpu.VMEM((experts, picks, sw), bf),
            dma((3,)),
            dma((2, n_tp)),
            dma((n_tp,)),
            dma,
            dma((n_tp,)),
            dma,
            dma,
            dma,
            dma((n_tp,)),
            dma,
            dma((GROUPS,)),
            dma,
            dma,
            pltpu.SemaphoreType.REGULAR((n_ep,)),
            pltpu.SemaphoreType.REGULAR,
        ],
        compiler_params=pltpu.CompilerParams(
            collective_id=0, has_side_effects=True, vmem_limit_bytes=32 * 1024 * 1024
        ),
    )(*(
        pltpu.with_memory_space_constraint(a, pltpu.HBM)
        for a in (tokens, chosen, chosen_weight, gate_weight, up_weight, down_weight)
    ))


def solution(mesh):
    return jax.shard_map(
        local,
        mesh=mesh,
        in_specs=(
            P("ep", None),
            P(),
            P("ep", None, None),
            P("ep", None, "tp"),
            P("ep", None, "tp"),
            P("ep", "tp", None),
        ),
        out_specs=P("ep", "tp"),
        check_vma=False,
    )
```

```python
import functools

import jax
import jax.numpy as jnp
from jax import lax
from jax.experimental import pallas as pl
from jax.experimental.pallas import tpu as pltpu
from jax.sharding import PartitionSpec as P

MESH = pl.DeviceIdType.MESH
GROUPS = 4
COLUMNS = 4
FAR = 2
EARLY = 2


def each(count, body):
    if count <= 8:
        for i in range(count):
            body(i)
    else:
        pl.loop(0, count)(body)


def kernel(
    n_ep, n_tp,
    tok_hbm, cho_hbm, wt_hbm, gate_hbm, up_hbm, down_hbm,
    out_ref,
    tok, cho, wt, gate, up, down,
    leaving, arrived, gate_acc, up_acc, place,
    part_out, part_in, first_in, back_out, back_in,
    in_sem, w_sem, d_sem,
    s1_send, s1_recv, hop_send, hop_recv, fan_send, fan_recv, s2_send, s2_recv, s3_send, s3_recv, first_send, first_recv,
    ep_ready, tp_seen, tp_ready,
):
    e = lax.axis_index("ep")
    t = lax.axis_index("tp")
    tok_count, width = tok.shape
    experts, picks = cho.shape
    rows = experts * picks
    sw = width // n_tp
    gs = n_ep // GROUPS
    mine = e // gs

    def group_at(i):
        if i == GROUPS - 1:
            return mine
        top = GROUPS - 1 - i
        down = GROUPS - i
        down = jnp.where(down > mine, down, down - 1) if i else 0
        up = jnp.where(i < mine, i, i + 1)
        return jnp.where(mine == 0, top, jnp.where(mine < GROUPS // 2, down, up))

    def direct(src, dst):
        return jnp.logical_or(
            jnp.logical_and(dst == 0, src >= FAR), jnp.logical_and(src == 0, dst > 0)
        )

    def quarter_at(i):
        if i == n_tp - 1:
            return t
        down_first = n_tp - 1 - i
        up_first = jnp.where(i < t, i, i + 1)
        return jnp.where(t == 0, down_first, up_first)

    barrier = pltpu.get_barrier_semaphore()

    def greet(p):
        pl.semaphore_signal(barrier, inc=1, device_id={"ep": p}, device_id_type=MESH)

    pl.loop(e + 1, n_ep)(greet)

    def greet_tp(p):
        pl.semaphore_signal(barrier, inc=1, device_id={"tp": p}, device_id_type=MESH)

    @pl.when(t == 0)
    def _():
        pl.loop(1, n_tp)(greet_tp)

    loads = [
        pltpu.make_async_copy(cho_hbm.at[e], cho, in_sem.at[0]),
        pltpu.make_async_copy(wt_hbm.at[0], wt, in_sem.at[1]),
        pltpu.make_async_copy(tok_hbm, tok, in_sem.at[2]),
    ]
    for c in loads:
        c.start()
    wloads = []
    for k in range(n_tp):
        piece = pl.ds(k * sw, sw)
        a = pltpu.make_async_copy(gate_hbm.at[0, piece, :], gate.at[piece, :], w_sem.at[0, k])
        b = pltpu.make_async_copy(up_hbm.at[0, piece, :], up.at[piece, :], w_sem.at[1, k])
        wloads.append((a, b))
    dloads = []
    for i in range(n_tp):
        col = pl.multiple_of(quarter_at(i) * sw, sw)
        dloads.append(
            pltpu.make_async_copy(down_hbm.at[0, :, pl.ds(col, sw)], down.at[i], d_sem.at[i])
        )

    with jax.named_scope("barrier"):
        floor = e + jnp.minimum(t, 1)

        @pl.when(floor > 0)
        def _():
            pl.semaphore_wait(barrier, floor)


    def answer(p):
        pl.semaphore_signal(ep_ready.at[e], inc=1, device_id={"ep": p}, device_id_type=MESH)

    pl.loop(0, e)(answer)

    @pl.when(t > 0)
    def _():
        pl.semaphore_signal(tp_seen, inc=1, device_id={"tp": 0}, device_id_type=MESH)

    with jax.named_scope("loadwait"):
        for c in loads:
            c.wait()
    for a, b in wloads:
        a.start()
        b.start()
    for c in dloads:
        c.start()

    lane = lax.broadcasted_iota(jnp.int32, (picks, picks), 1)
    sub = lax.broadcasted_iota(jnp.int32, (picks, picks), 0)
    diag = lane == sub
    position = lax.broadcasted_iota(jnp.int32, (picks, tok_count), 1).astype(jnp.float32)
    columns, hots = [], []
    for x in range(experts):
        spread = jnp.broadcast_to(cho[x : x + 1, :], (picks, picks)).astype(jnp.float32)
        column = jnp.sum(jnp.where(diag, spread, 0.0), axis=1, keepdims=True)
        columns.append(column)
        hots.append(jnp.where(position == column, 1.0, 0.0))
    onehot = jnp.concatenate(hots, axis=0).astype(jnp.bfloat16)
    with jax.named_scope("gather"):
        for k in range(n_tp):
            sel = jnp.dot(
                onehot, tok[:, k * sw : (k + 1) * sw], preferred_element_type=jnp.float32
            )
            leaving[k] = sel.reshape(experts, picks, sw).astype(jnp.bfloat16)

    def send_tokens(k, p):
        return pltpu.make_async_remote_copy(
            src_ref=leaving.at[k, p],
            dst_ref=arrived.at[k, e],
            send_sem=s1_send,
            recv_sem=s1_recv.at[k],
            device_id={"ep": p},
            device_id_type=MESH,
        )

    def send_hop(p):
        return pltpu.make_async_remote_copy(
            src_ref=leaving.at[t, p],
            dst_ref=arrived.at[t, e],
            send_sem=hop_send,
            recv_sem=hop_recv,
            device_id={"ep": p},
            device_id_type=MESH,
        )

    def send_group(g):
        for k in range(n_tp):
            each(gs, lambda i: send_tokens(k, g * gs + i).start())

    def ready_group(g):
        each(gs, lambda i: pl.semaphore_wait(ep_ready.at[g * gs + i], 1))

    with jax.named_scope("senddown"):
        pl.loop(0, mine)(send_group)

        def send_near(i):
            p = mine * gs + i

            @pl.when(p > e)
            def _():
                pl.semaphore_wait(ep_ready.at[p], 1)

            @pl.when(p != e)
            def _():
                for k in range(n_tp):
                    send_tokens(k, p).start()

        each(gs, send_near)
    with jax.named_scope("hop"):
        @pl.when(mine < GROUPS - 1)
        def _():
            ready_group(mine + 1)
            each(gs, lambda i: send_hop((mine + 1) * gs + i).start())

    with jax.named_scope("tpseen"):
        @pl.when(t == 0)
        def _():
            pl.semaphore_wait(tp_seen, n_tp - 1)

            def admit(p):
                pl.semaphore_signal(tp_ready, inc=1, device_id={"tp": p}, device_id_type=MESH)

            pl.loop(1, n_tp)(admit)

    with jax.named_scope("sendup"):
        def send_up(g):
            ready_group(g)
            send_group(g)

        pl.loop(mine + 2, GROUPS)(send_up)

    parts = []
    for x in range(experts):
        wide = jnp.broadcast_to(wt[x : x + 1, :], (picks, picks))
        wcol = jnp.sum(jnp.where(diag, wide, 0.0), axis=1, keepdims=True)
        parts.append(jnp.where(position == columns[x], wcol, 0.0))
    weighted = jnp.concatenate(parts, axis=0)
    hi = weighted.astype(jnp.bfloat16).astype(jnp.float32)
    mid = (weighted - hi).astype(jnp.bfloat16).astype(jnp.float32)
    lo = weighted - hi - mid
    place[...] = jnp.concatenate([hi, mid, lo], axis=0).T.astype(jnp.bfloat16)

    def landed(ref, sem):
        pltpu.make_async_copy(ref, ref, sem).wait()


    @pl.when(t > 0)
    def _():
        pl.semaphore_wait(tp_ready, 1)

    below = pl.ds((mine - 1) * gs, gs)

    def send_fan(i):
        return pltpu.make_async_remote_copy(
            src_ref=arrived.at[t, below],
            dst_ref=arrived.at[t, below],
            send_sem=fan_send,
            recv_sem=fan_recv.at[t],
            device_id={"tp": quarter_at(i)},
            device_id_type=MESH,
        )

    with jax.named_scope("fan"):
        @pl.when(mine > 0)
        def _():
            landed(arrived.at[t, pl.ds(0, gs)], hop_recv)
            for i in range(n_tp - 1):
                send_fan(i).start()

    for k in range(n_tp):
        arrived[k, e] = leaving[k, e]
    for a, b in wloads:
        a.wait()
        b.wait()
    for c in dloads:
        c.wait()
    hid = gate.shape[1]
    step = hid // COLUMNS
    hidden = []
    for k in range(n_tp):
        with jax.named_scope(f'tokin#k={k}'):
            @pl.when(mine == 0)
            def _():
                landed(arrived.at[k, pl.ds(0, n_ep - 1)], s1_recv.at[k])

            @pl.when(mine > 0)
            def _():
                landed(arrived.at[k, pl.ds(0, n_ep - 1 - gs)], s1_recv.at[k])

            @pl.when(jnp.logical_and(mine > 0, t != k))
            def _():
                landed(arrived.at[k, pl.ds(0, gs)], fan_recv.at[k])

        x = arrived[k].astype(jnp.float32).reshape(rows, sw).astype(jnp.bfloat16)
        deep = pl.ds(k * sw, sw)
        for c in range(COLUMNS):
            cols = pl.ds(c * step, step)
            g = jnp.dot(x, gate[deep, cols], preferred_element_type=jnp.float32)
            u = jnp.dot(x, up[deep, cols], preferred_element_type=jnp.float32)
            if k > 0:
                g += gate_acc[:, cols]
                u += up_acc[:, cols]
            if k < n_tp - 1:
                gate_acc[:, cols] = g
                up_acc[:, cols] = u
            else:
                hidden.append((g / (1.0 + jnp.exp(-g)) * u).astype(jnp.bfloat16))

    def send_part(i, gi):
        blocks = pl.ds(group_at(gi) * gs, gs)
        return pltpu.make_async_remote_copy(
            src_ref=part_out.at[i, blocks],
            dst_ref=part_in.at[t, blocks],
            send_sem=s2_send,
            recv_sem=s2_recv.at[gi],
            device_id={"tp": quarter_at(i)},
            device_id_type=MESH,
        )

    def start_part(i, gi):
        if i > 0:
            send_part(i, gi).start()
        else:
            @pl.when(jnp.logical_or(t == 0, jnp.logical_not(direct(mine, group_at(gi)))))
            def _():
                send_part(i, gi).start()

    def send_first(i, p):
        return pltpu.make_async_remote_copy(
            src_ref=part_out.at[i, p],
            dst_ref=first_in.at[t * n_ep + e],
            send_sem=first_send,
            recv_sem=first_recv,
            device_id={"ep": p, "tp": 0},
            device_id_type=MESH,
        )

    def start_first(i):
        @pl.when(mine >= FAR)
        def _():
            each(gs, lambda p: send_first(i, p).start())

        @pl.when(mine == 0)
        def _():
            each(n_ep - gs, lambda j: send_first(i, n_ep - 1 - j).start())

    def send_back(p):
        return pltpu.make_async_remote_copy(
            src_ref=back_out.at[p],
            dst_ref=back_in.at[e],
            send_sem=s3_send,
            recv_sem=s3_recv,
            device_id={"ep": p},
            device_id_type=MESH,
        )

    for i in range(n_tp):
        with jax.named_scope(f'down#i={i}'):
            part = jnp.dot(hidden[0], down[i, pl.ds(0, step)], preferred_element_type=jnp.float32)
            for c in range(1, COLUMNS):
                part += jnp.dot(
                    hidden[c], down[i, pl.ds(c * step, step)], preferred_element_type=jnp.float32
                )
            part_out[i] = part.reshape(experts, picks, sw).astype(jnp.bfloat16)
        if i == 0:
            @pl.when(t > 0)
            def _():
                start_first(0)
        if i < n_tp - 1:
            for gi in range(EARLY):
                start_part(i, gi)
        if i == n_tp - 2:
            for gi in range(EARLY, GROUPS):
                for x in range(n_tp - 1):
                    start_part(x, gi)

    @pl.when(t == 0)
    def _():
        start_first(n_tp - 1)

    for gi in range(GROUPS):
        gg = group_at(gi)

        @pl.when(jnp.logical_or(t > 0, jnp.logical_not(direct(mine, gg))))
        def _():
            blocks = pl.ds(gg * gs, gs)
            total = part_out[n_tp - 1, blocks].astype(jnp.float32)
            with jax.named_scope(f'rs#g={gi}'):
                landed(part_in.at[pl.ds(0, n_tp - 1), blocks], s2_recv.at[gi])
            for i in range(n_tp - 1):
                total += part_in[quarter_at(i), blocks].astype(jnp.float32)
            back_out[blocks] = total.astype(jnp.bfloat16)

            def give(i):
                p = gg * gs + i
                if gi < GROUPS - 1:
                    send_back(p).start()
                else:
                    @pl.when(p != e)
                    def _():
                        send_back(p).start()

            each(gs, give)

    near = FAR * gs
    back_in[e] = back_out[e]
    with jax.named_scope('backin'):
        @pl.when(t > 0)
        def _():
            landed(back_in.at[pl.ds(0, n_ep - 1)], s3_recv)

        @pl.when(jnp.logical_and(t == 0, mine == 0))
        def _():
            landed(back_in.at[pl.ds(0, near - 1)], s3_recv)

        @pl.when(jnp.logical_and(t == 0, mine > 0))
        def _():
            landed(back_in.at[pl.ds(0, n_ep - gs - 1)], s3_recv)

    def take_first(low, count):
        with jax.named_scope('firstin'):
            landed(first_in.at[pl.ds(0, n_tp * count)], first_recv)
        total = first_in[pl.ds(low, count)].astype(jnp.float32)
        for i in range(1, n_tp):
            total += first_in[pl.ds(i * n_ep + low, count)].astype(jnp.float32)
        back_in[pl.ds(low, count)] = total.astype(jnp.bfloat16)

    @pl.when(jnp.logical_and(t == 0, mine == 0))
    def _():
        take_first(near, n_ep - near)

    @pl.when(jnp.logical_and(t == 0, mine > 0))
    def _():
        take_first(0, gs)

    with jax.named_scope("combine"):
        y = back_in[...].astype(jnp.float32).reshape(rows, sw).astype(jnp.bfloat16)
        y = jnp.concatenate([y, y, y], axis=0)
        result = jnp.dot(place[...], y, preferred_element_type=jnp.float32)
        out_ref[...] = result.astype(out_ref.dtype)

    with jax.named_scope("drain"):
        for k in range(n_tp):
            @pl.when(mine == GROUPS - 1)
            def _():
                landed(leaving.at[k, pl.ds(0, n_ep - 1)], s1_send)

            @pl.when(mine < GROUPS - 1)
            def _():
                landed(leaving.at[k, pl.ds(0, n_ep - 1 - gs)], s1_send)

        @pl.when(mine < GROUPS - 1)
        def _():
            landed(leaving.at[0, pl.ds(0, gs)], hop_send)

        @pl.when(mine > 0)
        def _():
            landed(arrived.at[pl.ds(0, n_tp - 1), pl.ds(0, gs)], fan_send)

        def sent(rows_out, parts_out, backs_out):
            if rows_out:
                landed(first_in.at[pl.ds(0, rows_out)], first_send)
            landed(first_in.at[pl.ds(0, parts_out)], s2_send)
            landed(back_out.at[pl.ds(0, backs_out)], s3_send)

        parts = (n_tp - 1) * n_ep
        for low, high, rows_out in ((0, 1, n_ep - gs), (1, FAR, 0), (FAR, GROUPS, gs)):
            here = jnp.logical_and(mine >= low, mine < high)

            @pl.when(jnp.logical_and(here, t == 0))
            def _():
                sent(rows_out, parts, n_ep - 1 - rows_out)

            @pl.when(jnp.logical_and(here, t > 0))
            def _():
                sent(rows_out, parts - rows_out, n_ep - 1)


def local(tokens, chosen, chosen_weight, gate_weight, up_weight, down_weight):
    n_ep, n_tp = lax.axis_size("ep"), lax.axis_size("tp")
    tok_count, width = tokens.shape
    blocks, experts, picks = chosen.shape
    hid = gate_weight.shape[2]
    rows = blocks * picks
    sw = width // n_tp
    bf, f32 = jnp.bfloat16, jnp.float32
    dma = pltpu.SemaphoreType.DMA
    hbm = pl.BlockSpec(memory_space=pltpu.HBM)
    return pl.pallas_call(
        functools.partial(kernel, n_ep, n_tp),
        out_shape=jax.ShapeDtypeStruct((tok_count, sw), bf),
        in_specs=[hbm] * 6,
        out_specs=pl.BlockSpec(memory_space=pltpu.VMEM),
        scratch_shapes=[
            pltpu.VMEM((tok_count, width), bf),
            pltpu.VMEM((experts, picks), jnp.int32),
            pltpu.VMEM((experts, picks), f32),
            pltpu.VMEM((width, hid), bf),
            pltpu.VMEM((width, hid), bf),
            pltpu.VMEM((n_tp, hid, sw), bf),
            pltpu.VMEM((n_tp, experts, picks, sw), bf),
            pltpu.VMEM((n_tp, blocks, picks, sw), bf),
            pltpu.VMEM((rows, hid), f32),
            pltpu.VMEM((rows, hid), f32),
            pltpu.VMEM((tok_count, 3 * experts * picks), bf),
            pltpu.VMEM((n_tp, blocks, picks, sw), bf),
            pltpu.VMEM((n_tp, blocks, picks, sw), bf),
            pltpu.VMEM((n_tp * n_ep, picks, sw), bf),
            pltpu.VMEM((blocks, picks, sw), bf),
            pltpu.VMEM((experts, picks, sw), bf),
            dma((3,)),
            dma((2, n_tp)),
            dma((n_tp,)),
            dma,
            dma((n_tp,)),
            dma,
            dma,
            dma,
            dma((n_tp,)),
            dma,
            dma((GROUPS,)),
            dma,
            dma,
            dma,
            dma,
            pltpu.SemaphoreType.REGULAR((n_ep,)),
            pltpu.SemaphoreType.REGULAR,
            pltpu.SemaphoreType.REGULAR,
        ],
        compiler_params=pltpu.CompilerParams(
            collective_id=0, has_side_effects=True, vmem_limit_bytes=32 * 1024 * 1024
        ),
    )(*(
        pltpu.with_memory_space_constraint(a, pltpu.HBM)
        for a in (tokens, chosen, chosen_weight, gate_weight, up_weight, down_weight)
    ))


def solution(mesh):
    return jax.shard_map(
        local,
        mesh=mesh,
        in_specs=(
            P("ep", None),
            P(),
            P("ep", None, None),
            P("ep", None, "tp"),
            P("ep", None, "tp"),
            P("ep", "tp", None),
        ),
        out_specs=P("ep", "tp"),
        check_vma=False,
    )
```

```python
import functools

import jax
import jax.numpy as jnp
from jax import lax
from jax.experimental import pallas as pl
from jax.experimental.pallas import tpu as pltpu
from jax.sharding import PartitionSpec as P

MESH = pl.DeviceIdType.MESH
GROUPS = 4
COLUMNS = 4
FAR = 2
OFFSETS = (-1, 1, -2, 2)
EARLY = 2


def each(count, body):
    if count <= 8:
        for i in range(count):
            body(i)
    else:
        pl.loop(0, count)(body)


def kernel(
    n_ep, n_tp,
    tok_hbm, cho_hbm, wt_hbm, gate_hbm, up_hbm, down_hbm,
    out_ref,
    tok, cho, wt, gate, up, down,
    leaving, arrived, gate_acc, up_acc, place,
    part_out, part_in, first_in, back_out, back_in,
    in_sem, w_sem,
    s1_send, s1_recv, hop_send, hop_recv, fan_send, fan_recv, s2_send, s2_recv, s3_send, s3_recv, first_send, first_recv,
    ep_ready, tp_seen, tp_ready,
):
    e = lax.axis_index("ep")
    t = lax.axis_index("tp")
    tok_count, width = tok.shape
    experts, picks = cho.shape
    rows = experts * picks
    sw = width // n_tp
    gs = n_ep // GROUPS
    mine = e // gs

    def group_at(i):
        if i == GROUPS - 1:
            return mine
        top = GROUPS - 1 - i
        down = GROUPS - i
        down = jnp.where(down > mine, down, down - 1) if i else 0
        up = jnp.where(i < mine, i, i + 1)
        return jnp.where(mine == 0, top, jnp.where(mine < GROUPS // 2, down, up))

    def is_first(i):
        if i == 0:
            return t > 0
        return t == 0 if i == n_tp - 1 else t < 0

    def direct(i, src, dst):
        near = jnp.logical_or(dst == 0, src == 0)
        near = jnp.logical_and(near, dst != src)
        far = jnp.logical_and(dst == 0, src >= FAR)
        return jnp.where(is_first(i), near, far)

    def quarter_at(i):
        if i == n_tp - 1:
            return t
        down_first = n_tp - 1 - i
        up_first = jnp.where(i < t, i, i + 1)
        return jnp.where(t == 0, down_first, up_first)

    barrier = pltpu.get_barrier_semaphore()

    def greet(p):
        pl.semaphore_signal(barrier, inc=1, device_id={"ep": p}, device_id_type=MESH)

    pl.loop(e + 1, n_ep)(greet)

    def greet_tp(p):
        pl.semaphore_signal(barrier, inc=1, device_id={"tp": p}, device_id_type=MESH)

    @pl.when(t == 0)
    def _():
        pl.loop(1, n_tp)(greet_tp)

    loads = [
        pltpu.make_async_copy(cho_hbm.at[e], cho, in_sem.at[0]),
        pltpu.make_async_copy(wt_hbm.at[0], wt, in_sem.at[1]),
        pltpu.make_async_copy(tok_hbm, tok, in_sem.at[2]),
    ]
    for c in loads:
        c.start()
    wloads = []
    for i in range(n_tp):
        deep = pl.ds(i * sw, sw)
        col = pl.multiple_of(quarter_at(i) * sw, sw)
        wloads += [
            pltpu.make_async_copy(gate_hbm.at[0, deep, :], gate.at[deep, :], w_sem),
            pltpu.make_async_copy(up_hbm.at[0, deep, :], up.at[deep, :], w_sem),
            pltpu.make_async_copy(down_hbm.at[0, :, pl.ds(col, sw)], down.at[i], w_sem),
        ]

    with jax.named_scope("barrier"):
        floor = e + jnp.minimum(t, 1)

        @pl.when(floor > 0)
        def _():
            pl.semaphore_wait(barrier, floor)


    def answer(p):
        pl.semaphore_signal(ep_ready.at[e], inc=1, device_id={"ep": p}, device_id_type=MESH)

    pl.loop(0, e)(answer)

    @pl.when(t > 0)
    def _():
        pl.semaphore_signal(tp_seen, inc=1, device_id={"tp": 0}, device_id_type=MESH)

    with jax.named_scope("loadwait"):
        for c in loads:
            c.wait()
    for c in wloads:
        c.start()

    lane = lax.broadcasted_iota(jnp.int32, (picks, picks), 1)
    sub = lax.broadcasted_iota(jnp.int32, (picks, picks), 0)
    diag = lane == sub
    position = lax.broadcasted_iota(jnp.int32, (picks, tok_count), 1).astype(jnp.float32)
    columns, hots = [], []
    for x in range(experts):
        spread = jnp.broadcast_to(cho[x : x + 1, :], (picks, picks)).astype(jnp.float32)
        column = jnp.sum(jnp.where(diag, spread, 0.0), axis=1, keepdims=True)
        columns.append(column)
        hots.append(jnp.where(position == column, 1.0, 0.0))
    onehot = jnp.concatenate(hots, axis=0).astype(jnp.bfloat16)
    with jax.named_scope("gather"):
        for k in range(n_tp):
            sel = jnp.dot(
                onehot, tok[:, k * sw : (k + 1) * sw], preferred_element_type=jnp.float32
            )
            leaving[k] = sel.reshape(experts, picks, sw).astype(jnp.bfloat16)

    def send_tokens(k, p):
        return pltpu.make_async_remote_copy(
            src_ref=leaving.at[k, p],
            dst_ref=arrived.at[k, e],
            send_sem=s1_send,
            recv_sem=s1_recv.at[k],
            device_id={"ep": p},
            device_id_type=MESH,
        )

    def send_hop(slot, p):
        return pltpu.make_async_remote_copy(
            src_ref=leaving.at[t, p],
            dst_ref=arrived.at[t, e],
            send_sem=hop_send,
            recv_sem=hop_recv.at[slot],
            device_id={"ep": p},
            device_id_type=MESH,
        )

    def hop_group(slot, g):
        each(gs, lambda i: send_hop(slot, g * gs + i).start())

    def hop_odd(slot, g):
        each(gs // 2, lambda i: send_hop(slot, g * gs + 2 * i + 1).start())

    def send_even(g):
        for k in range(n_tp):
            each(gs // 2, lambda i: send_tokens(k, g * gs + 2 * i).start())

    def send_group(g):
        for k in range(n_tp):
            each(gs, lambda i: send_tokens(k, g * gs + i).start())

    def ready_group(g):
        each(gs, lambda i: pl.semaphore_wait(ep_ready.at[g * gs + i], 1))

    with jax.named_scope("senddown"):
        @pl.when(mine > 0)
        def _():
            hop_group(1, mine - 1)

        @pl.when(mine > 1)
        def _():
            hop_odd(3, mine - 2)

        pl.loop(0, mine - 2)(send_group)

        @pl.when(mine > 1)
        def _():
            send_even(mine - 2)


        def send_near(i):
            p = mine * gs + i

            @pl.when(p > e)
            def _():
                pl.semaphore_wait(ep_ready.at[p], 1)

            @pl.when(p != e)
            def _():
                for k in range(n_tp):
                    send_tokens(k, p).start()

        each(gs, send_near)
    with jax.named_scope("hop"):
        @pl.when(mine < GROUPS - 1)
        def _():
            ready_group(mine + 1)
            hop_group(0, mine + 1)

    with jax.named_scope("tpseen"):
        @pl.when(t == 0)
        def _():
            pl.semaphore_wait(tp_seen, n_tp - 1)

            def admit(p):
                pl.semaphore_signal(tp_ready, inc=1, device_id={"tp": p}, device_id_type=MESH)

            pl.loop(1, n_tp)(admit)

    with jax.named_scope("sendup"):
        def send_up(g):
            ready_group(g)
            send_group(g)

        @pl.when(mine == 0)
        def _():
            ready_group(2)
            hop_odd(2, 2)
            send_even(2)

        pl.loop(jnp.maximum(mine + 2, 3), GROUPS)(send_up)

    parts = []
    for x in range(experts):
        wide = jnp.broadcast_to(wt[x : x + 1, :], (picks, picks))
        wcol = jnp.sum(jnp.where(diag, wide, 0.0), axis=1, keepdims=True)
        parts.append(jnp.where(position == columns[x], wcol, 0.0))
    weighted = jnp.concatenate(parts, axis=0)
    hi = weighted.astype(jnp.bfloat16).astype(jnp.float32)
    mid = (weighted - hi).astype(jnp.bfloat16).astype(jnp.float32)
    lo = weighted - hi - mid
    place[...] = jnp.concatenate([hi, mid, lo], axis=0).T.astype(jnp.bfloat16)

    def landed(ref, sem):
        pltpu.make_async_copy(ref, ref, sem).wait()


    @pl.when(t > 0)
    def _():
        pl.semaphore_wait(tp_ready, 1)

    odd = lax.rem(e, 2)
    both = jnp.logical_and(mine > 0, mine < GROUPS - 1)

    def split_from(slot):
        src = mine + OFFSETS[slot]
        near = jnp.logical_and(src >= 0, src < GROUPS)
        if slot < 2:
            return near
        if slot == 2:
            near = src == 0
        return jnp.logical_and(near, odd == 1)

    def send_fan(slot, i):
        blocks = pl.ds((mine + OFFSETS[slot]) * gs, gs)
        return pltpu.make_async_remote_copy(
            src_ref=arrived.at[t, blocks],
            dst_ref=arrived.at[t, blocks],
            send_sem=fan_send,
            recv_sem=fan_recv.at[t],
            device_id={"tp": quarter_at(i)},
            device_id_type=MESH,
        )

    with jax.named_scope("fan"):
        for slot in range(4):
            @pl.when(split_from(slot))
            def _():
                landed(arrived.at[t, pl.ds(0, gs)], hop_recv.at[slot])
                for i in range(n_tp - 1):
                    send_fan(slot, i).start()

    for k in range(n_tp):
        arrived[k, e] = leaving[k, e]
    landed(gate, w_sem)
    landed(up, w_sem)
    landed(down, w_sem)
    hid = gate.shape[1]
    step = hid // COLUMNS
    hidden = []
    for k in range(n_tp):
        with jax.named_scope(f'tokin#k={k}'):
            for sides in (1, 2):
                for parity in (0, 1):
                    here = both if sides == 2 else jnp.logical_not(both)
                    more = jnp.logical_and(odd == 1, mine < GROUPS - 1)
                    here = jnp.logical_and(here, more == (parity == 1))

                    @pl.when(here)
                    def _():
                        split = gs * (sides + parity)
                        landed(arrived.at[k, pl.ds(0, n_ep - 1 - split)], s1_recv.at[k])

                        @pl.when(t != k)
                        def _():
                            landed(arrived.at[k, pl.ds(0, split)], fan_recv.at[k])

        x = arrived[k].astype(jnp.float32).reshape(rows, sw).astype(jnp.bfloat16)
        deep = pl.ds(k * sw, sw)
        for c in range(COLUMNS):
            cols = pl.ds(c * step, step)
            g = jnp.dot(x, gate[deep, cols], preferred_element_type=jnp.float32)
            u = jnp.dot(x, up[deep, cols], preferred_element_type=jnp.float32)
            if k > 0:
                g += gate_acc[:, cols]
                u += up_acc[:, cols]
            if k < n_tp - 1:
                gate_acc[:, cols] = g
                up_acc[:, cols] = u
            else:
                hidden.append((g / (1.0 + jnp.exp(-g)) * u).astype(jnp.bfloat16))

    def send_part(i, gi):
        blocks = pl.ds(group_at(gi) * gs, gs)
        return pltpu.make_async_remote_copy(
            src_ref=part_out.at[i, blocks],
            dst_ref=part_in.at[t, blocks],
            send_sem=s2_send,
            recv_sem=s2_recv.at[gi],
            device_id={"tp": quarter_at(i)},
            device_id_type=MESH,
        )

    def start_part(i, gi):
        @pl.when(jnp.logical_not(direct(i, mine, group_at(gi))))
        def _():
            send_part(i, gi).start()

    def send_first(i, p):
        return pltpu.make_async_remote_copy(
            src_ref=part_out.at[i, p],
            dst_ref=first_in.at[t * n_ep + e],
            send_sem=first_send,
            recv_sem=first_recv,
            device_id={"ep": p, "tp": quarter_at(i)},
            device_id_type=MESH,
        )

    def start_first(i):
        @pl.when(jnp.logical_and(direct(i, mine, 0), mine > 0))
        def _():
            each(gs, lambda p: send_first(i, p).start())

        @pl.when(jnp.logical_and(is_first(i), mine == 0))
        def _():
            each(n_ep - gs, lambda j: send_first(i, n_ep - 1 - j).start())

    def send_back(p):
        return pltpu.make_async_remote_copy(
            src_ref=back_out.at[p],
            dst_ref=back_in.at[e],
            send_sem=s3_send,
            recv_sem=s3_recv,
            device_id={"ep": p},
            device_id_type=MESH,
        )

    for i in range(n_tp):
        with jax.named_scope(f'down#i={i}'):
            part = jnp.dot(hidden[0], down[i, pl.ds(0, step)], preferred_element_type=jnp.float32)
            for c in range(1, COLUMNS):
                part += jnp.dot(
                    hidden[c], down[i, pl.ds(c * step, step)], preferred_element_type=jnp.float32
                )
            part_out[i] = part.reshape(experts, picks, sw).astype(jnp.bfloat16)
        if i == 0:
            @pl.when(jnp.logical_and(t > 0, mine == 0))
            def _():
                send_part(0, GROUPS - 1).start()
        start_first(i)
        if i < n_tp - 1:
            for gi in range(EARLY):
                start_part(i, gi)
        if i == n_tp - 2:
            for gi in range(EARLY, GROUPS):
                for x in range(n_tp - 1):
                    if x or gi < GROUPS - 1:
                        start_part(x, gi)
                    else:
                        @pl.when(jnp.logical_or(t == 0, mine > 0))
                        def _():
                            start_part(x, gi)

    for gi in range(GROUPS):
        gg = group_at(gi)

        @pl.when(jnp.logical_not(direct(n_tp - 1, mine, gg)))
        def _():
            blocks = pl.ds(gg * gs, gs)
            total = part_out[n_tp - 1, blocks].astype(jnp.float32)
            with jax.named_scope(f'rs#g={gi}'):
                landed(part_in.at[pl.ds(0, n_tp - 1), blocks], s2_recv.at[gi])
            for i in range(n_tp - 1):
                total += part_in[quarter_at(i), blocks].astype(jnp.float32)
            back_out[blocks] = total.astype(jnp.bfloat16)

            def give(i):
                p = gg * gs + i
                if gi < GROUPS - 1:
                    send_back(p).start()
                else:
                    @pl.when(p != e)
                    def _():
                        send_back(p).start()

            each(gs, give)

    back_in[e] = back_out[e]

    def take_first(low, count):
        with jax.named_scope('firstin'):
            landed(first_in.at[pl.ds(0, n_tp * count)], first_recv)
        total = first_in[pl.ds(low, count)].astype(jnp.float32)
        for i in range(1, n_tp):
            total += first_in[pl.ds(i * n_ep + low, count)].astype(jnp.float32)
        back_in[pl.ds(low, count)] = total.astype(jnp.bfloat16)

    for here, low, count in (
        (jnp.logical_and(t == 0, mine == 0), gs, n_ep - gs),
        (jnp.logical_and(t == 0, mine > 0), 0, gs),
        (jnp.logical_and(t > 0, mine == 0), FAR * gs, n_ep - FAR * gs),
        (jnp.logical_and(t > 0, mine > 0), 0, 0),
    ):
        @pl.when(here)
        def _():
            with jax.named_scope('backin'):
                landed(back_in.at[pl.ds(0, n_ep - 1 - count)], s3_recv)
            if count:
                take_first(low, count)

    with jax.named_scope("combine"):
        y = back_in[...].astype(jnp.float32).reshape(rows, sw).astype(jnp.bfloat16)
        y = jnp.concatenate([y, y, y], axis=0)
        result = jnp.dot(place[...], y, preferred_element_type=jnp.float32)
        out_ref[...] = result.astype(out_ref.dtype)

    with jax.named_scope("drain"):
        def sent_tokens(hops):
            for k in range(n_tp):
                landed(leaving.at[k, pl.ds(0, n_ep - 1 - hops)], s1_send)
            landed(leaving.at[0, pl.ds(0, hops)], hop_send)

        @pl.when(jnp.logical_not(both))
        def _():
            sent_tokens(gs + gs // 2)

        @pl.when(mine == 1)
        def _():
            sent_tokens(2 * gs)

        @pl.when(jnp.logical_and(both, mine > 1))
        def _():
            sent_tokens(2 * gs + gs // 2)

        for slot in range(4):
            @pl.when(split_from(slot))
            def _():
                landed(arrived.at[pl.ds(0, n_tp - 1), pl.ds(0, gs)], fan_send)

        def sent(firsts, parts, backs):
            if firsts:
                landed(first_in.at[pl.ds(0, firsts)], first_send)
            landed(first_in.at[pl.ds(0, parts)], s2_send)
            landed(back_out.at[pl.ds(0, backs)], s3_send)

        for low, high in ((0, 1), (1, FAR), (FAR, GROUPS)):
            here = jnp.logical_and(mine >= low, mine < high)
            lead = gs if low else n_ep - gs
            rest = gs if low == FAR else 0
            firsts = lead + (n_tp - 1) * rest

            @pl.when(jnp.logical_and(here, t == 0))
            def _():
                sent(firsts, (n_tp - 1) * (n_ep - rest), n_ep - 1 - lead)

            @pl.when(jnp.logical_and(here, t > 0))
            def _():
                parts = n_ep - lead + (n_tp - 2) * (n_ep - rest)
                sent(firsts, parts, n_ep - 1 - rest)


def local(tokens, chosen, chosen_weight, gate_weight, up_weight, down_weight):
    n_ep, n_tp = lax.axis_size("ep"), lax.axis_size("tp")
    tok_count, width = tokens.shape
    blocks, experts, picks = chosen.shape
    hid = gate_weight.shape[2]
    rows = blocks * picks
    sw = width // n_tp
    bf, f32 = jnp.bfloat16, jnp.float32
    dma = pltpu.SemaphoreType.DMA
    hbm = pl.BlockSpec(memory_space=pltpu.HBM)
    return pl.pallas_call(
        functools.partial(kernel, n_ep, n_tp),
        out_shape=jax.ShapeDtypeStruct((tok_count, sw), bf),
        in_specs=[hbm] * 6,
        out_specs=pl.BlockSpec(memory_space=pltpu.VMEM),
        scratch_shapes=[
            pltpu.VMEM((tok_count, width), bf),
            pltpu.VMEM((experts, picks), jnp.int32),
            pltpu.VMEM((experts, picks), f32),
            pltpu.VMEM((width, hid), bf),
            pltpu.VMEM((width, hid), bf),
            pltpu.VMEM((n_tp, hid, sw), bf),
            pltpu.VMEM((n_tp, experts, picks, sw), bf),
            pltpu.VMEM((n_tp, blocks, picks, sw), bf),
            pltpu.VMEM((rows, hid), f32),
            pltpu.VMEM((rows, hid), f32),
            pltpu.VMEM((tok_count, 3 * experts * picks), bf),
            pltpu.VMEM((n_tp, blocks, picks, sw), bf),
            pltpu.VMEM((n_tp, blocks, picks, sw), bf),
            pltpu.VMEM((n_tp * n_ep, picks, sw), bf),
            pltpu.VMEM((blocks, picks, sw), bf),
            pltpu.VMEM((experts, picks, sw), bf),
            dma((3,)),
            dma,
            dma,
            dma((n_tp,)),
            dma,
            dma((4,)),
            dma,
            dma((n_tp,)),
            dma,
            dma((GROUPS,)),
            dma,
            dma,
            dma,
            dma,
            pltpu.SemaphoreType.REGULAR((n_ep,)),
            pltpu.SemaphoreType.REGULAR,
            pltpu.SemaphoreType.REGULAR,
        ],
        compiler_params=pltpu.CompilerParams(
            collective_id=0, has_side_effects=True, vmem_limit_bytes=32 * 1024 * 1024
        ),
    )(*(
        pltpu.with_memory_space_constraint(a, pltpu.HBM)
        for a in (tokens, chosen, chosen_weight, gate_weight, up_weight, down_weight)
    ))


def solution(mesh):
    return jax.shard_map(
        local,
        mesh=mesh,
        in_specs=(
            P("ep", None),
            P(),
            P("ep", None, None),
            P("ep", None, "tp"),
            P("ep", None, "tp"),
            P("ep", "tp", None),
        ),
        out_specs=P("ep", "tp"),
        check_vma=False,
    )
```

```python
import functools

import jax
import jax.numpy as jnp
from jax import lax
from jax.experimental import pallas as pl
from jax.experimental.pallas import tpu as pltpu
from jax.sharding import PartitionSpec as P

MESH = pl.DeviceIdType.MESH
GROUPS = 4
COLUMNS = 4
FIRST = ((1, 0), (2, 0), (3, 0), (0, 1), (0, 2), (0, 3))
EVERY = ((2, 0), (3, 0), (3, 1), (0, 2), (0, 3))
SPLIT = (((1, 2), (2, 1)), ((1, 2), (2, 1), (0, 2), (2, 0)))
EARLY = 2


def each(count, body):
    if count <= 8:
        for i in range(count):
            body(i)
    else:
        pl.loop(0, count)(body)


def kernel(
    n_ep, n_tp,
    tok_hbm, cho_hbm, wt_hbm, gate_hbm, up_hbm, down_hbm,
    out_ref,
    tok, cho, wt, gate, up, down,
    leaving, arrived, gate_acc, up_acc, place,
    part_out, part_in, first_in, back_out, back_in,
    in_sem, w_sem,
    s1_send, s1_recv, hop_send, hop_recv, fan_send, s2_send, s2_recv, s3_send, s3_recv, first_send, first_recv,
    ep_ready, tp_seen, tp_ready, tp_above,
):
    e = lax.axis_index("ep")
    t = lax.axis_index("tp")
    tok_count, width = tok.shape
    experts, picks = cho.shape
    rows = experts * picks
    sw = width // n_tp
    gs = n_ep // GROUPS
    mine = e // gs

    def group_at(i):
        if i == GROUPS - 1:
            return mine
        top = GROUPS - 1 - i
        down = GROUPS - i
        down = jnp.where(down > mine, down, down - 1) if i else 0
        up = jnp.where(i < mine, i, i + 1)
        return jnp.where(mine == 0, top, jnp.where(mine < GROUPS // 2, down, up))

    def any_of(terms):
        out = mine < 0
        for term in terms:
            out = jnp.logical_or(out, term)
        return out

    def direct(i, dst):
        pairs = EVERY if i else FIRST
        return any_of(jnp.logical_and(mine == a, dst == b) for a, b in pairs)

    def quarter_at(i):
        if i == 0:
            return 0
        others = t if i == n_tp - 1 else jnp.where(i < t, i, i + 1)
        return jnp.where(t == 0, n_tp - i, others)

    def leaves(i):
        if i == 0:
            return t > 0
        return t == 0 if i == n_tp - 1 else t >= 0

    own_at = jnp.where(t == 0, 0, n_tp - 1)

    def slice_at(i):
        return lax.rem(t + i, n_tp)

    barrier = pltpu.get_barrier_semaphore()

    def greet(p):
        pl.semaphore_signal(barrier, inc=1, device_id={"ep": p}, device_id_type=MESH)

    pl.loop(e + 1, n_ep)(greet)

    def greet_tp(p):
        pl.semaphore_signal(barrier, inc=1, device_id={"tp": p}, device_id_type=MESH)

    @pl.when(t == 0)
    def _():
        pl.loop(1, n_tp)(greet_tp)

    loads = [
        pltpu.make_async_copy(cho_hbm.at[e], cho, in_sem.at[0]),
        pltpu.make_async_copy(wt_hbm.at[0], wt, in_sem.at[1]),
        pltpu.make_async_copy(tok_hbm, tok, in_sem.at[2]),
    ]
    for c in loads:
        c.start()
    wloads = []
    for i in range(n_tp):
        deep = pl.ds(pl.multiple_of(slice_at(i) * sw, sw), sw)
        col = pl.multiple_of(quarter_at(i) * sw, sw)
        wloads += [
            pltpu.make_async_copy(gate_hbm.at[0, deep, :], gate.at[deep, :], w_sem),
            pltpu.make_async_copy(up_hbm.at[0, deep, :], up.at[deep, :], w_sem),
            pltpu.make_async_copy(down_hbm.at[0, :, pl.ds(col, sw)], down.at[i], w_sem),
        ]

    with jax.named_scope("barrier"):
        floor = e + jnp.minimum(t, 1)

        @pl.when(floor > 0)
        def _():
            pl.semaphore_wait(barrier, floor)


    def answer(p):
        pl.semaphore_signal(ep_ready.at[e], inc=1, device_id={"ep": p}, device_id_type=MESH)

    pl.loop(0, e)(answer)

    @pl.when(t > 0)
    def _():
        pl.semaphore_signal(tp_seen, inc=1, device_id={"tp": 0}, device_id_type=MESH)

    with jax.named_scope("loadwait"):
        for c in loads:
            c.wait()
    for c in wloads:
        c.start()

    lane = lax.broadcasted_iota(jnp.int32, (picks, picks), 1)
    sub = lax.broadcasted_iota(jnp.int32, (picks, picks), 0)
    diag = lane == sub
    position = lax.broadcasted_iota(jnp.int32, (picks, tok_count), 1).astype(jnp.float32)
    columns, hots = [], []
    for x in range(experts):
        spread = jnp.broadcast_to(cho[x : x + 1, :], (picks, picks)).astype(jnp.float32)
        column = jnp.sum(jnp.where(diag, spread, 0.0), axis=1, keepdims=True)
        columns.append(column)
        hots.append(jnp.where(position == column, 1.0, 0.0))
    onehot = jnp.concatenate(hots, axis=0).astype(jnp.bfloat16)
    with jax.named_scope("gather"):
        for k in range(n_tp):
            sel = jnp.dot(
                onehot, tok[:, k * sw : (k + 1) * sw], preferred_element_type=jnp.float32
            )
            leaving[k] = sel.reshape(experts, picks, sw).astype(jnp.bfloat16)

    def send_tokens(k, p):
        return pltpu.make_async_remote_copy(
            src_ref=leaving.at[k, p],
            dst_ref=arrived.at[k, e],
            send_sem=s1_send,
            recv_sem=s1_recv.at[k],
            device_id={"ep": p},
            device_id_type=MESH,
        )

    def send_hop(slot, p):
        return pltpu.make_async_remote_copy(
            src_ref=leaving.at[t, p],
            dst_ref=arrived.at[t, e],
            send_sem=hop_send,
            recv_sem=hop_recv.at[slot],
            device_id={"ep": p},
            device_id_type=MESH,
        )

    odd = lax.rem(e, 2)

    def split_to(parity, dst):
        return any_of([mine == a for a, b in SPLIT[parity] if b == dst])

    def split_from(src):
        return any_of(
            jnp.logical_and(mine == b, odd == parity)
            for parity in range(2)
            for a, b in SPLIT[parity]
            if a == src
        )

    def hops_to(dst):
        for parity in range(2):
            for a, b in SPLIT[parity]:
                if b == dst:
                    @pl.when(mine == a)
                    def _():
                        each(gs // 2, lambda i: send_hop(a, b * gs + 2 * i + parity).start())

    def direct_to(dst):
        @pl.when(jnp.logical_not(split_to(1, dst)))
        def _():
            for i in range(n_tp):
                k = slice_at(i)
                each(gs, lambda j: send_tokens(k, dst * gs + j).start())

        @pl.when(jnp.logical_and(split_to(1, dst), jnp.logical_not(split_to(0, dst))))
        def _():
            for i in range(n_tp):
                k = slice_at(i)
                each(gs // 2, lambda j: send_tokens(k, dst * gs + 2 * j).start())

    def ready_group(g):
        each(gs, lambda i: pl.semaphore_wait(ep_ready.at[g * gs + i], 1))

    with jax.named_scope("senddown"):
        for dst in range(GROUPS - 2, -1, -1):
            @pl.when(mine > dst)
            def _():
                hops_to(dst)

        for dst in range(GROUPS - 1):
            @pl.when(mine > dst)
            def _():
                direct_to(dst)

        def send_near(i):
            p = mine * gs + i
            p = jnp.where(p < e, p, p + 1)

            @pl.when(p > e)
            def _():
                pl.semaphore_wait(ep_ready.at[p], 1)

            for k in range(n_tp):
                send_tokens(k, p).start()

        each(gs - 1, send_near)
    with jax.named_scope("hop"):
        for dst in range(1, GROUPS):
            @pl.when(mine == dst - 1)
            def _():
                ready_group(dst)
                hops_to(dst)
                direct_to(dst)

    with jax.named_scope("tpseen"):
        @pl.when(t == 0)
        def _():
            pl.semaphore_wait(tp_seen, n_tp - 1)

            def admit(p):
                pl.semaphore_signal(tp_ready, inc=1, device_id={"tp": p}, device_id_type=MESH)

            pl.loop(1, n_tp)(admit)

    with jax.named_scope("sendup"):
        for dst in range(2, GROUPS):
            @pl.when(mine < dst - 1)
            def _():
                ready_group(dst)
                hops_to(dst)
                direct_to(dst)

    parts = []
    for x in range(experts):
        wide = jnp.broadcast_to(wt[x : x + 1, :], (picks, picks))
        wcol = jnp.sum(jnp.where(diag, wide, 0.0), axis=1, keepdims=True)
        parts.append(jnp.where(position == columns[x], wcol, 0.0))
    weighted = jnp.concatenate(parts, axis=0)
    hi = weighted.astype(jnp.bfloat16).astype(jnp.float32)
    mid = (weighted - hi).astype(jnp.bfloat16).astype(jnp.float32)
    lo = weighted - hi - mid
    place[...] = jnp.concatenate([hi, mid, lo], axis=0).T.astype(jnp.bfloat16)

    def landed(ref, sem):
        pltpu.make_async_copy(ref, ref, sem).wait()


    @pl.when(t > 0)
    def _():
        pl.semaphore_wait(tp_ready, 1)

    @pl.when(mine == 0)
    def _():
        for i in range(n_tp - 1):
            pl.semaphore_signal(
                tp_above, inc=1, device_id={"tp": lax.rem(t + 1 + i, n_tp)}, device_id_type=MESH
            )

    def send_fan(slot, i):
        blocks = pl.ds(slot * gs, gs)
        return pltpu.make_async_remote_copy(
            src_ref=arrived.at[t, blocks],
            dst_ref=arrived.at[t, blocks],
            send_sem=fan_send,
            recv_sem=s1_recv.at[t],
            device_id={"tp": lax.rem(t + 1 + i, n_tp)},
            device_id_type=MESH,
        )

    with jax.named_scope("fan"):
        for slot in range(GROUPS):
            @pl.when(split_from(slot))
            def _():
                landed(arrived.at[t, pl.ds(0, gs)], hop_recv.at[slot])
                for i in range(n_tp - 1):
                    send_fan(slot, i).start()

    heard = {}
    for group in range(GROUPS):
        for parity in range(2):
            count = gs * sum(b == group for _, b in SPLIT[parity])
            case = jnp.logical_and(mine == group, odd == parity)
            heard[count] = jnp.logical_or(heard[count], case) if count in heard else case

    for k in range(n_tp):
        arrived[k, e] = leaving[k, e]
    @pl.when(mine == 0)
    def _():
        pl.semaphore_wait(tp_above, n_tp - 1)

    landed(gate, w_sem)
    landed(up, w_sem)
    landed(down, w_sem)
    hid = gate.shape[1]
    step = hid // COLUMNS
    hidden = []
    for i in range(n_tp):
        k = slice_at(i)
        with jax.named_scope(f'tokin#k={i}'):
            if i:
                landed(arrived.at[k, pl.ds(0, n_ep - 1)], s1_recv.at[k])
            else:
                for count in sorted(heard):
                    @pl.when(heard[count])
                    def _():
                        landed(arrived.at[k, pl.ds(0, n_ep - 1 - count)], s1_recv.at[k])

        x = arrived[k].astype(jnp.float32).reshape(rows, sw).astype(jnp.bfloat16)
        deep = pl.ds(pl.multiple_of(k * sw, sw), sw)
        for c in range(COLUMNS):
            cols = pl.ds(c * step, step)
            g = jnp.dot(x, gate[deep, cols], preferred_element_type=jnp.float32)
            u = jnp.dot(x, up[deep, cols], preferred_element_type=jnp.float32)
            if i > 0:
                g += gate_acc[:, cols]
                u += up_acc[:, cols]
            if i < n_tp - 1:
                gate_acc[:, cols] = g
                up_acc[:, cols] = u
            else:
                hidden.append((g / (1.0 + jnp.exp(-g)) * u).astype(jnp.bfloat16))

    def send_part(i, gi):
        blocks = pl.ds(group_at(gi) * gs, gs)
        return pltpu.make_async_remote_copy(
            src_ref=part_out.at[i, blocks],
            dst_ref=part_in.at[t, blocks],
            send_sem=s2_send,
            recv_sem=s2_recv.at[gi],
            device_id={"tp": quarter_at(i)},
            device_id_type=MESH,
        )

    def start_part(i, gi, when):
        @pl.when(jnp.logical_and(when, jnp.logical_not(direct(i, group_at(gi)))))
        def _():
            send_part(i, gi).start()

    def send_first(i, p):
        return pltpu.make_async_remote_copy(
            src_ref=part_out.at[i, p],
            dst_ref=first_in.at[t * n_ep + e],
            send_sem=first_send,
            recv_sem=first_recv,
            device_id={"ep": p, "tp": quarter_at(i)},
            device_id_type=MESH,
        )

    def start_first(i):
        for dst in (0, *range(GROUPS - 1, 0, -1)):
            @pl.when(direct(i, dst))
            def _():
                each(gs, lambda j: send_first(i, dst * gs + j).start())

    def send_back(p):
        return pltpu.make_async_remote_copy(
            src_ref=back_out.at[p],
            dst_ref=back_in.at[e],
            send_sem=s3_send,
            recv_sem=s3_recv,
            device_id={"ep": p},
            device_id_type=MESH,
        )

    for i in range(n_tp):
        with jax.named_scope(f'down#i={i}'):
            part = jnp.dot(hidden[0], down[i, pl.ds(0, step)], preferred_element_type=jnp.float32)
            for c in range(1, COLUMNS):
                part += jnp.dot(
                    hidden[c], down[i, pl.ds(c * step, step)], preferred_element_type=jnp.float32
                )
            part_out[i] = part.reshape(experts, picks, sw).astype(jnp.bfloat16)
        if i == 0:
            start_part(0, GROUPS - 1, jnp.logical_and(t > 0, mine == 0))
        start_first(i)
        here = leaves(i)
        if i < n_tp - 1:
            for gi in range(EARLY):
                start_part(i, gi, here)
            for gi in range(EARLY, GROUPS - 1):
                start_part(i, gi, jnp.logical_and(here, mine != 1))
        else:
            for gi in range(GROUPS):
                start_part(i, gi, here)
        if i == n_tp - 2:
            for gi in range(EARLY, GROUPS):
                for x in range(n_tp - 1):
                    late = mine == 1 if gi < GROUPS - 1 else mine > (0 if x == 0 else -1)
                    start_part(x, gi, jnp.logical_and(leaves(x), late))

    for gi in range(GROUPS):
        gg = group_at(gi)

        ended = jnp.where(t == 0, direct(0, gg), direct(1, gg))

        @pl.when(jnp.logical_not(ended))
        def _():
            blocks = pl.ds(gg * gs, gs)
            total = part_out[own_at, blocks].astype(jnp.float32)
            with jax.named_scope(f'rs#g={gi}'):
                landed(part_in.at[pl.ds(0, n_tp - 1), blocks], s2_recv.at[gi])
            for i in range(n_tp - 1):
                total += part_in[lax.rem(t + 1 + i, n_tp), blocks].astype(jnp.float32)
            back_out[blocks] = total.astype(jnp.bfloat16)

            def give(i):
                p = gg * gs + i
                if gi < GROUPS - 1:
                    send_back(p).start()
                else:
                    @pl.when(p != e)
                    def _():
                        send_back(p).start()

            each(gs, give)

    back_in[e] = back_out[e]
    with jax.named_scope("drain"):
        for group in range(GROUPS):
            @pl.when(mine == group)
            def _():
                hops = gs // 2 * sum(a == group for pairs in SPLIT for a, _ in pairs)
                for k in range(n_tp):
                    landed(leaving.at[k, pl.ds(0, n_ep - 1 - hops)], s1_send)
                if hops:
                    landed(leaving.at[0, pl.ds(0, hops)], hop_send)

        for slot in range(GROUPS):
            @pl.when(split_from(slot))
            def _():
                landed(arrived.at[pl.ds(0, n_tp - 1), pl.ds(0, gs)], fan_send)

        def sent(lead, rest):
            firsts = gs * (lead + (n_tp - 1) * rest)
            if firsts:
                landed(first_in.at[pl.ds(0, firsts)], first_send)

            @pl.when(t == 0)
            def _():
                parts = (n_tp - 1) * (n_ep - gs * rest)
                landed(first_in.at[pl.ds(0, parts)], s2_send)
                landed(back_out.at[pl.ds(0, n_ep - 1 - gs * lead)], s3_send)

            @pl.when(t > 0)
            def _():
                parts = n_ep - gs * lead + (n_tp - 2) * (n_ep - gs * rest)
                landed(first_in.at[pl.ds(0, parts)], s2_send)
                landed(back_out.at[pl.ds(0, n_ep - 1 - gs * rest)], s3_send)

        for group in range(GROUPS):
            @pl.when(mine == group)
            def _():
                sent(sum(a == group for a, _ in FIRST), sum(a == group for a, _ in EVERY))

    ends = {}
    for group in range(GROUPS):
        for pairs, here in ((FIRST, t == 0), (EVERY, t > 0)):
            case = jnp.logical_and(mine == group, here)
            come = tuple(sorted(a for a, b in pairs if b == group))
            ends[come] = jnp.logical_or(ends[come], case) if come in ends else case

    for come in sorted(ends):
        @pl.when(ends[come])
        def _():
            with jax.named_scope('backin'):
                landed(back_in.at[pl.ds(0, n_ep - 1 - gs * len(come))], s3_recv)
            if come:
                with jax.named_scope('firstin'):
                    landed(first_in.at[pl.ds(0, n_tp * gs * len(come))], first_recv)
            for src in come:
                total = first_in[pl.ds(src * gs, gs)].astype(jnp.float32)
                for i in range(1, n_tp):
                    total += first_in[pl.ds(i * n_ep + src * gs, gs)].astype(jnp.float32)
                back_in[pl.ds(src * gs, gs)] = total.astype(jnp.bfloat16)

    with jax.named_scope("combine"):
        y = back_in[...].astype(jnp.float32).reshape(rows, sw).astype(jnp.bfloat16)
        y = jnp.concatenate([y, y, y], axis=0)
        result = jnp.dot(place[...], y, preferred_element_type=jnp.float32)
        out_ref[...] = result.astype(out_ref.dtype)


def local(tokens, chosen, chosen_weight, gate_weight, up_weight, down_weight):
    n_ep, n_tp = lax.axis_size("ep"), lax.axis_size("tp")
    tok_count, width = tokens.shape
    blocks, experts, picks = chosen.shape
    hid = gate_weight.shape[2]
    rows = blocks * picks
    sw = width // n_tp
    bf, f32 = jnp.bfloat16, jnp.float32
    dma = pltpu.SemaphoreType.DMA
    hbm = pl.BlockSpec(memory_space=pltpu.HBM)
    return pl.pallas_call(
        functools.partial(kernel, n_ep, n_tp),
        out_shape=jax.ShapeDtypeStruct((tok_count, sw), bf),
        in_specs=[hbm] * 6,
        out_specs=pl.BlockSpec(memory_space=pltpu.VMEM),
        scratch_shapes=[
            pltpu.VMEM((tok_count, width), bf),
            pltpu.VMEM((experts, picks), jnp.int32),
            pltpu.VMEM((experts, picks), f32),
            pltpu.VMEM((width, hid), bf),
            pltpu.VMEM((width, hid), bf),
            pltpu.VMEM((n_tp, hid, sw), bf),
            pltpu.VMEM((n_tp, experts, picks, sw), bf),
            pltpu.VMEM((n_tp, blocks, picks, sw), bf),
            pltpu.VMEM((rows, hid), f32),
            pltpu.VMEM((rows, hid), f32),
            pltpu.VMEM((tok_count, 3 * experts * picks), bf),
            pltpu.VMEM((n_tp, blocks, picks, sw), bf),
            pltpu.VMEM((n_tp, blocks, picks, sw), bf),
            pltpu.VMEM((n_tp * n_ep, picks, sw), bf),
            pltpu.VMEM((blocks, picks, sw), bf),
            pltpu.VMEM((experts, picks, sw), bf),
            dma((3,)),
            dma,
            dma,
            dma((n_tp,)),
            dma,
            dma((GROUPS,)),
            dma,
            dma,
            dma((GROUPS,)),
            dma,
            dma,
            dma,
            dma,
            pltpu.SemaphoreType.REGULAR((n_ep,)),
            pltpu.SemaphoreType.REGULAR,
            pltpu.SemaphoreType.REGULAR,
            pltpu.SemaphoreType.REGULAR,
        ],
        compiler_params=pltpu.CompilerParams(
            collective_id=0, has_side_effects=True, vmem_limit_bytes=32 * 1024 * 1024
        ),
    )(*(
        pltpu.with_memory_space_constraint(a, pltpu.HBM)
        for a in (tokens, chosen, chosen_weight, gate_weight, up_weight, down_weight)
    ))


def solution(mesh):
    return jax.shard_map(
        local,
        mesh=mesh,
        in_specs=(
            P("ep", None),
            P(),
            P("ep", None, None),
            P("ep", None, "tp"),
            P("ep", None, "tp"),
            P("ep", "tp", None),
        ),
        out_specs=P("ep", "tp"),
        check_vma=False,
    )
```

```python
import functools

import jax
import jax.numpy as jnp
from jax import lax
from jax.experimental import pallas as pl
from jax.experimental.pallas import tpu as pltpu
from jax.sharding import PartitionSpec as P

MESH = pl.DeviceIdType.MESH
GROUPS = 4
COLUMNS = 4
FIRST = ((1, 0), (2, 0), (3, 0), (0, 1), (0, 2), (0, 3))
EVERY = ((2, 0), (3, 0), (3, 1), (0, 2), (0, 3), (1, 0))
SPLIT = (((1, 2), (2, 1)), ((1, 2), (2, 1), (0, 2), (2, 0)))
EARLY = 2


def each(count, body):
    if count <= 8:
        for i in range(count):
            body(i)
    else:
        pl.loop(0, count)(body)


def kernel(
    n_ep, n_tp,
    tok_hbm, cho_hbm, wt_hbm, gate_hbm, up_hbm, down_hbm,
    out_ref,
    tok, cho, wt, gate, up, down,
    leaving, arrived, gate_acc, up_acc, place,
    part_out, part_in, first_in, back_out, back_in,
    in_sem, w_sem,
    s1_send, s1_recv, hop_send, hop_recv, fan_send, s2_send, s2_recv, s3_send, s3_recv, first_send, first_recv,
    ep_ready, tp_seen, tp_ready, tp_above,
):
    e = lax.axis_index("ep")
    t = lax.axis_index("tp")
    tok_count, width = tok.shape
    experts, picks = cho.shape
    rows = experts * picks
    sw = width // n_tp
    gs = n_ep // GROUPS
    mine = e // gs

    def group_at(i):
        if i == GROUPS - 1:
            return mine
        top = GROUPS - 1 - i
        down = GROUPS - i
        down = jnp.where(down > mine, down, down - 1) if i else 0
        up = jnp.where(i < mine, i, i + 1)
        return jnp.where(mine == 0, top, jnp.where(mine < GROUPS // 2, down, up))

    def any_of(terms):
        out = mine < 0
        for term in terms:
            out = jnp.logical_or(out, term)
        return out

    def direct(i, dst):
        pairs = EVERY if i else FIRST
        return any_of(jnp.logical_and(mine == a, dst == b) for a, b in pairs)

    def quarter_at(i):
        if i == 0:
            return 0
        others = t if i == n_tp - 1 else jnp.where(i < t, i, i + 1)
        return jnp.where(t == 0, n_tp - i, others)

    def leaves(i):
        if i == 0:
            return t > 0
        return t == 0 if i == n_tp - 1 else t >= 0

    own_at = jnp.where(t == 0, 0, n_tp - 1)

    def slice_at(i):
        return lax.rem(t + i, n_tp)

    barrier = pltpu.get_barrier_semaphore()

    def greet(p):
        pl.semaphore_signal(barrier, inc=1, device_id={"ep": p}, device_id_type=MESH)

    pl.loop(e + 1, n_ep)(greet)

    @pl.when(mine == GROUPS - 1)
    def _():
        each(gs, greet)


    def greet_tp(p):
        pl.semaphore_signal(barrier, inc=1, device_id={"tp": p}, device_id_type=MESH)

    @pl.when(t == 0)
    def _():
        pl.loop(1, n_tp)(greet_tp)

    loads = [
        pltpu.make_async_copy(cho_hbm.at[e], cho, in_sem.at[0]),
        pltpu.make_async_copy(wt_hbm.at[0], wt, in_sem.at[1]),
        pltpu.make_async_copy(tok_hbm, tok, in_sem.at[2]),
    ]
    for c in loads:
        c.start()
    wloads = []
    for i in range(n_tp):
        deep = pl.ds(pl.multiple_of(slice_at(i) * sw, sw), sw)
        col = pl.multiple_of(quarter_at(i) * sw, sw)
        wloads += [
            pltpu.make_async_copy(gate_hbm.at[0, deep, :], gate.at[deep, :], w_sem),
            pltpu.make_async_copy(up_hbm.at[0, deep, :], up.at[deep, :], w_sem),
            pltpu.make_async_copy(down_hbm.at[0, :, pl.ds(col, sw)], down.at[i], w_sem),
        ]

    with jax.named_scope("barrier"):
        floor = e + jnp.minimum(t, 1)

        @pl.when(mine > 0)
        def _():
            pl.semaphore_wait(barrier, floor)


    def answer(p):
        pl.semaphore_signal(ep_ready.at[e], inc=1, device_id={"ep": p}, device_id_type=MESH)

    @pl.when(mine > 0)
    def _():
        pl.loop(jnp.where(mine == GROUPS - 1, gs, 0), e)(answer)

    @pl.when(jnp.logical_and(t > 0, mine > 0))
    def _():
        pl.semaphore_signal(tp_seen, inc=1, device_id={"tp": 0}, device_id_type=MESH)

    with jax.named_scope("loadwait"):
        for c in loads:
            c.wait()
    for c in wloads:
        c.start()

    lane = lax.broadcasted_iota(jnp.int32, (picks, picks), 1)
    sub = lax.broadcasted_iota(jnp.int32, (picks, picks), 0)
    diag = lane == sub
    position = lax.broadcasted_iota(jnp.int32, (picks, tok_count), 1).astype(jnp.float32)
    columns, hots = [], []
    for x in range(experts):
        spread = jnp.broadcast_to(cho[x : x + 1, :], (picks, picks)).astype(jnp.float32)
        column = jnp.sum(jnp.where(diag, spread, 0.0), axis=1, keepdims=True)
        columns.append(column)
        hots.append(jnp.where(position == column, 1.0, 0.0))
    onehot = jnp.concatenate(hots, axis=0).astype(jnp.bfloat16)
    with jax.named_scope("gather"):
        for k in range(n_tp):
            sel = jnp.dot(
                onehot, tok[:, k * sw : (k + 1) * sw], preferred_element_type=jnp.float32
            )
            leaving[k] = sel.reshape(experts, picks, sw).astype(jnp.bfloat16)

    def send_tokens(k, p):
        return pltpu.make_async_remote_copy(
            src_ref=leaving.at[k, p],
            dst_ref=arrived.at[k, e],
            send_sem=s1_send,
            recv_sem=s1_recv.at[k],
            device_id={"ep": p},
            device_id_type=MESH,
        )

    def send_hop(slot, p):
        return pltpu.make_async_remote_copy(
            src_ref=leaving.at[t, p],
            dst_ref=arrived.at[t, e],
            send_sem=hop_send,
            recv_sem=hop_recv.at[slot],
            device_id={"ep": p},
            device_id_type=MESH,
        )

    odd = lax.rem(e, 2)

    def split_to(parity, dst):
        return any_of([mine == a for a, b in SPLIT[parity] if b == dst])

    def split_from(src):
        return any_of(
            jnp.logical_and(mine == b, odd == parity)
            for parity in range(2)
            for a, b in SPLIT[parity]
            if a == src
        )

    def hops_to(dst):
        for parity in range(2):
            for a, b in SPLIT[parity]:
                if b == dst:
                    @pl.when(mine == a)
                    def _():
                        each(gs // 2, lambda i: send_hop(a, b * gs + 2 * i + parity).start())

    def direct_to(dst):
        @pl.when(jnp.logical_not(split_to(1, dst)))
        def _():
            for i in range(n_tp):
                k = slice_at(i)
                each(gs, lambda j: send_tokens(k, dst * gs + j).start())

        @pl.when(jnp.logical_and(split_to(1, dst), jnp.logical_not(split_to(0, dst))))
        def _():
            for i in range(n_tp):
                k = slice_at(i)
                each(gs // 2, lambda j: send_tokens(k, dst * gs + 2 * j).start())

    def ready_group(g):
        each(gs, lambda i: pl.semaphore_wait(ep_ready.at[g * gs + i], 1))

    with jax.named_scope("senddown"):
        for dst in range(GROUPS - 2, -1, -1):
            @pl.when(mine > dst)
            def _():
                hops_to(dst)

        for dst in range(GROUPS - 1):
            @pl.when(mine > dst)
            def _():
                direct_to(dst)

        def send_near(i):
            p = mine * gs + i
            p = jnp.where(p < e, p, p + 1)

            @pl.when(p > e)
            def _():
                pl.semaphore_wait(ep_ready.at[p], 1)

            for k in range(n_tp):
                send_tokens(k, p).start()

        @pl.when(mine > 0)
        def _():
            each(gs - 1, send_near)

    with jax.named_scope("hop"):
        for dst in range(1, GROUPS):
            @pl.when(mine == dst - 1)
            def _():
                ready_group(dst)
                hops_to(dst)
                direct_to(dst)

    with jax.named_scope("tpseen"):
        def open_tp():
            pl.semaphore_wait(tp_seen, n_tp - 1)

            def admit(p):
                pl.semaphore_signal(tp_ready, inc=1, device_id={"tp": p}, device_id_type=MESH)

            pl.loop(1, n_tp)(admit)

        @pl.when(jnp.logical_and(t == 0, mine > 0))
        def _():
            open_tp()

    with jax.named_scope("sendup"):
        for dst in range(2, GROUPS):
            @pl.when(mine < dst - 1)
            def _():
                if dst < GROUPS - 1:
                    ready_group(dst)
                else:
                    @pl.when(mine == 0)
                    def _():
                        pl.semaphore_wait(barrier, floor + gs)

                    @pl.when(mine > 0)
                    def _():
                        ready_group(dst)

                hops_to(dst)
                direct_to(dst)

        @pl.when(mine == 0)
        def _():
            pl.loop(0, e)(answer)

            @pl.when(t > 0)
            def _():
                pl.semaphore_signal(tp_seen, inc=1, device_id={"tp": 0}, device_id_type=MESH)

            each(gs - 1, send_near)

            @pl.when(t == 0)
            def _():
                open_tp()


    parts = []
    for x in range(experts):
        wide = jnp.broadcast_to(wt[x : x + 1, :], (picks, picks))
        wcol = jnp.sum(jnp.where(diag, wide, 0.0), axis=1, keepdims=True)
        parts.append(jnp.where(position == columns[x], wcol, 0.0))
    weighted = jnp.concatenate(parts, axis=0)
    hi = weighted.astype(jnp.bfloat16).astype(jnp.float32)
    mid = weighted - hi
    place[...] = jnp.concatenate([hi, mid], axis=0).T.astype(jnp.bfloat16)

    def landed(ref, sem):
        pltpu.make_async_copy(ref, ref, sem).wait()


    @pl.when(t > 0)
    def _():
        pl.semaphore_wait(tp_ready, 1)

    @pl.when(mine == 0)
    def _():
        for i in range(n_tp - 1):
            pl.semaphore_signal(
                tp_above, inc=1, device_id={"tp": lax.rem(t + 1 + i, n_tp)}, device_id_type=MESH
            )

    def send_fan(slot, i):
        blocks = pl.ds(slot * gs, gs)
        return pltpu.make_async_remote_copy(
            src_ref=arrived.at[t, blocks],
            dst_ref=arrived.at[t, blocks],
            send_sem=fan_send,
            recv_sem=s1_recv.at[t],
            device_id={"tp": lax.rem(t + 1 + i, n_tp)},
            device_id_type=MESH,
        )

    with jax.named_scope("fan"):
        for slot in range(GROUPS):
            @pl.when(split_from(slot))
            def _():
                landed(arrived.at[t, pl.ds(0, gs)], hop_recv.at[slot])
                for i in range(n_tp - 1):
                    send_fan(slot, i).start()

    heard = {}
    for group in range(GROUPS):
        for parity in range(2):
            count = gs * sum(b == group for _, b in SPLIT[parity])
            case = jnp.logical_and(mine == group, odd == parity)
            heard[count] = jnp.logical_or(heard[count], case) if count in heard else case

    for k in range(n_tp):
        arrived[k, e] = leaving[k, e]
    @pl.when(mine == 0)
    def _():
        pl.semaphore_wait(tp_above, n_tp - 1)

    landed(gate, w_sem)
    landed(up, w_sem)
    landed(down, w_sem)
    hid = gate.shape[1]
    step = hid // COLUMNS
    hidden = []
    for i in range(n_tp):
        k = slice_at(i)
        with jax.named_scope(f'tokin#k={i}'):
            if i:
                landed(arrived.at[k, pl.ds(0, n_ep - 1)], s1_recv.at[k])
            else:
                for count in sorted(heard):
                    @pl.when(heard[count])
                    def _():
                        landed(arrived.at[k, pl.ds(0, n_ep - 1 - count)], s1_recv.at[k])

        x = arrived[k].astype(jnp.float32).reshape(rows, sw).astype(jnp.bfloat16)
        deep = pl.ds(pl.multiple_of(k * sw, sw), sw)
        for c in range(COLUMNS):
            cols = pl.ds(c * step, step)
            g = jnp.dot(x, gate[deep, cols], preferred_element_type=jnp.float32)
            u = jnp.dot(x, up[deep, cols], preferred_element_type=jnp.float32)
            if i > 0:
                g += gate_acc[:, cols]
                u += up_acc[:, cols]
            if i < n_tp - 1:
                gate_acc[:, cols] = g
                up_acc[:, cols] = u
            else:
                hidden.append((g / (1.0 + jnp.exp(-g)) * u).astype(jnp.bfloat16))

    def send_part(i, gi):
        blocks = pl.ds(group_at(gi) * gs, gs)
        return pltpu.make_async_remote_copy(
            src_ref=part_out.at[i, blocks],
            dst_ref=part_in.at[t, blocks],
            send_sem=s2_send,
            recv_sem=s2_recv.at[gi],
            device_id={"tp": quarter_at(i)},
            device_id_type=MESH,
        )

    def start_part(i, gi, when):
        @pl.when(jnp.logical_and(when, jnp.logical_not(direct(i, group_at(gi)))))
        def _():
            send_part(i, gi).start()

    def send_first(i, p):
        return pltpu.make_async_remote_copy(
            src_ref=part_out.at[i, p],
            dst_ref=first_in.at[t * n_ep + e],
            send_sem=first_send,
            recv_sem=first_recv,
            device_id={"ep": p, "tp": quarter_at(i)},
            device_id_type=MESH,
        )

    def start_first(i):
        for dst in (0, *range(GROUPS - 1, 0, -1)):
            @pl.when(direct(i, dst))
            def _():
                each(gs, lambda j: send_first(i, dst * gs + j).start())

    def send_back(p):
        return pltpu.make_async_remote_copy(
            src_ref=back_out.at[p],
            dst_ref=back_in.at[e],
            send_sem=s3_send,
            recv_sem=s3_recv,
            device_id={"ep": p},
            device_id_type=MESH,
        )

    for i in range(n_tp):
        with jax.named_scope(f'down#i={i}'):
            part = jnp.dot(hidden[0], down[i, pl.ds(0, step)], preferred_element_type=jnp.float32)
            for c in range(1, COLUMNS):
                part += jnp.dot(
                    hidden[c], down[i, pl.ds(c * step, step)], preferred_element_type=jnp.float32
                )
            part_out[i] = part.reshape(experts, picks, sw).astype(jnp.bfloat16)
        if i == 0:
            start_part(0, GROUPS - 1, jnp.logical_and(t > 0, mine == 0))
        start_first(i)
        here = leaves(i)
        if i < n_tp - 1:
            for gi in range(EARLY):
                start_part(i, gi, here)
            for gi in range(EARLY, GROUPS - 1):
                start_part(i, gi, here)
        else:
            for gi in range(GROUPS):
                start_part(i, gi, here)
        if i == n_tp - 2:
            for gi in range(EARLY, GROUPS):
                for x in range(n_tp - 1):
                    late = mine < 0 if gi < GROUPS - 1 else mine > (0 if x == 0 else -1)
                    start_part(x, gi, jnp.logical_and(leaves(x), late))

    for gi in range(GROUPS):
        gg = group_at(gi)

        ended = jnp.where(t == 0, direct(0, gg), direct(1, gg))

        @pl.when(jnp.logical_not(ended))
        def _():
            blocks = pl.ds(gg * gs, gs)
            total = part_out[own_at, blocks].astype(jnp.float32)
            with jax.named_scope(f'rs#g={gi}'):
                landed(part_in.at[pl.ds(0, n_tp - 1), blocks], s2_recv.at[gi])
            for i in range(n_tp - 1):
                total += part_in[lax.rem(t + 1 + i, n_tp), blocks].astype(jnp.float32)
            back_out[blocks] = total.astype(jnp.bfloat16)

            def give(i):
                p = gg * gs + i
                if gi < GROUPS - 1:
                    send_back(p).start()
                else:
                    @pl.when(p != e)
                    def _():
                        send_back(p).start()

            each(gs, give)

    back_in[e] = back_out[e]
    with jax.named_scope("drain"):
        for group in range(GROUPS):
            @pl.when(mine == group)
            def _():
                hops = gs // 2 * sum(a == group for pairs in SPLIT for a, _ in pairs)
                for k in range(n_tp):
                    landed(leaving.at[k, pl.ds(0, n_ep - 1 - hops)], s1_send)
                if hops:
                    landed(leaving.at[0, pl.ds(0, hops)], hop_send)

        for slot in range(GROUPS):
            @pl.when(split_from(slot))
            def _():
                landed(arrived.at[pl.ds(0, n_tp - 1), pl.ds(0, gs)], fan_send)

        def sent(lead, rest):
            firsts = gs * (lead + (n_tp - 1) * rest)
            if firsts:
                landed(first_in.at[pl.ds(0, firsts)], first_send)

            @pl.when(t == 0)
            def _():
                parts = (n_tp - 1) * (n_ep - gs * rest)
                landed(first_in.at[pl.ds(0, parts)], s2_send)
                landed(back_out.at[pl.ds(0, n_ep - 1 - gs * lead)], s3_send)

            @pl.when(t > 0)
            def _():
                parts = n_ep - gs * lead + (n_tp - 2) * (n_ep - gs * rest)
                landed(first_in.at[pl.ds(0, parts)], s2_send)
                landed(back_out.at[pl.ds(0, n_ep - 1 - gs * rest)], s3_send)

        for group in range(GROUPS):
            @pl.when(mine == group)
            def _():
                sent(sum(a == group for a, _ in FIRST), sum(a == group for a, _ in EVERY))

    ends = {}
    for group in range(GROUPS):
        for pairs, here in ((FIRST, t == 0), (EVERY, t > 0)):
            case = jnp.logical_and(mine == group, here)
            come = tuple(sorted(a for a, b in pairs if b == group))
            ends[come] = jnp.logical_or(ends[come], case) if come in ends else case

    for come in sorted(ends):
        @pl.when(ends[come])
        def _():
            with jax.named_scope('backin'):
                landed(back_in.at[pl.ds(0, n_ep - 1 - gs * len(come))], s3_recv)
            if come:
                with jax.named_scope('firstin'):
                    landed(first_in.at[pl.ds(0, n_tp * gs * len(come))], first_recv)
            for src in come:
                total = first_in[pl.ds(src * gs, gs)].astype(jnp.float32)
                for i in range(1, n_tp):
                    total += first_in[pl.ds(i * n_ep + src * gs, gs)].astype(jnp.float32)
                back_in[pl.ds(src * gs, gs)] = total.astype(jnp.bfloat16)

    with jax.named_scope("combine"):
        y = back_in[...].astype(jnp.float32).reshape(rows, sw).astype(jnp.bfloat16)
        y = jnp.concatenate([y, y], axis=0)
        result = jnp.dot(place[...], y, preferred_element_type=jnp.float32)
        out_ref[...] = result.astype(out_ref.dtype)


def local(tokens, chosen, chosen_weight, gate_weight, up_weight, down_weight):
    n_ep, n_tp = lax.axis_size("ep"), lax.axis_size("tp")
    tok_count, width = tokens.shape
    blocks, experts, picks = chosen.shape
    hid = gate_weight.shape[2]
    rows = blocks * picks
    sw = width // n_tp
    bf, f32 = jnp.bfloat16, jnp.float32
    dma = pltpu.SemaphoreType.DMA
    hbm = pl.BlockSpec(memory_space=pltpu.HBM)
    return pl.pallas_call(
        functools.partial(kernel, n_ep, n_tp),
        out_shape=jax.ShapeDtypeStruct((tok_count, sw), bf),
        in_specs=[hbm] * 6,
        out_specs=pl.BlockSpec(memory_space=pltpu.VMEM),
        scratch_shapes=[
            pltpu.VMEM((tok_count, width), bf),
            pltpu.VMEM((experts, picks), jnp.int32),
            pltpu.VMEM((experts, picks), f32),
            pltpu.VMEM((width, hid), bf),
            pltpu.VMEM((width, hid), bf),
            pltpu.VMEM((n_tp, hid, sw), bf),
            pltpu.VMEM((n_tp, experts, picks, sw), bf),
            pltpu.VMEM((n_tp, blocks, picks, sw), bf),
            pltpu.VMEM((rows, hid), f32),
            pltpu.VMEM((rows, hid), f32),
            pltpu.VMEM((tok_count, 2 * experts * picks), bf),
            pltpu.VMEM((n_tp, blocks, picks, sw), bf),
            pltpu.VMEM((n_tp, blocks, picks, sw), bf),
            pltpu.VMEM((n_tp * n_ep, picks, sw), bf),
            pltpu.VMEM((blocks, picks, sw), bf),
            pltpu.VMEM((experts, picks, sw), bf),
            dma((3,)),
            dma,
            dma,
            dma((n_tp,)),
            dma,
            dma((GROUPS,)),
            dma,
            dma,
            dma((GROUPS,)),
            dma,
            dma,
            dma,
            dma,
            pltpu.SemaphoreType.REGULAR((n_ep,)),
            pltpu.SemaphoreType.REGULAR,
            pltpu.SemaphoreType.REGULAR,
            pltpu.SemaphoreType.REGULAR,
        ],
        compiler_params=pltpu.CompilerParams(
            collective_id=0, has_side_effects=True, vmem_limit_bytes=32 * 1024 * 1024
        ),
    )(*(
        pltpu.with_memory_space_constraint(a, pltpu.HBM)
        for a in (tokens, chosen, chosen_weight, gate_weight, up_weight, down_weight)
    ))


def solution(mesh):
    return jax.shard_map(
        local,
        mesh=mesh,
        in_specs=(
            P("ep", None),
            P(),
            P("ep", None, None),
            P("ep", None, "tp"),
            P("ep", None, "tp"),
            P("ep", "tp", None),
        ),
        out_specs=P("ep", "tp"),
        check_vma=False,
    )
```

```python
import functools

import jax
import jax.numpy as jnp
from jax import lax
from jax.experimental import pallas as pl
from jax.experimental.pallas import tpu as pltpu
from jax.sharding import PartitionSpec as P

MESH = pl.DeviceIdType.MESH
GROUPS = 4
COLUMNS = 4
FIRST = ((1, 0), (2, 0), (3, 0), (0, 1), (0, 2), (0, 3))
EVERY = ((2, 0), (3, 0), (3, 1), (0, 2), (0, 3), (1, 0))
SPLIT = (((1, 2), (2, 1)), ((1, 2), (2, 1), (0, 2), (2, 0)))
EARLY = 2


def each(count, body):
    if count <= 8:
        for i in range(count):
            body(i)
    else:
        pl.loop(0, count)(body)


def kernel(
    n_ep, n_tp,
    tok_hbm, cho_hbm, wt_hbm, gate_hbm, up_hbm, down_hbm,
    out_ref,
    tok, cho, wt, gate, up, down,
    leaving, arrived, gate_acc, up_acc, place,
    part_out, part_in, first_in, back_out, back_in,
    in_sem, w_sem,
    s1_send, s1_recv, hop_send, hop_recv, fan_send, s2_send, s2_recv, s3_send, s3_recv, first_send, first_recv,
    ep_ready, tp_seen, tp_ready, tp_above,
):
    e = lax.axis_index("ep")
    t = lax.axis_index("tp")
    tok_count, width = tok.shape
    experts, picks = cho.shape
    rows = experts * picks
    sw = width // n_tp
    gs = n_ep // GROUPS
    mine = e // gs

    def group_at(i):
        if i == GROUPS - 1:
            return mine
        top = GROUPS - 1 - i
        down = GROUPS - i
        down = jnp.where(down > mine, down, down - 1) if i else 0
        up = jnp.where(i < mine, i, i + 1)
        return jnp.where(mine == 0, top, jnp.where(mine < GROUPS // 2, down, up))

    def any_of(terms):
        out = mine < 0
        for term in terms:
            out = jnp.logical_or(out, term)
        return out

    def direct(i, dst):
        pairs = EVERY if i else FIRST
        return any_of(jnp.logical_and(mine == a, dst == b) for a, b in pairs)

    def quarter_at(i):
        if i == 0:
            return 0
        others = t if i == n_tp - 1 else jnp.where(i < t, i, i + 1)
        return jnp.where(t == 0, n_tp - i, others)

    def leaves(i):
        if i == 0:
            return t > 0
        return t == 0 if i == n_tp - 1 else t >= 0

    own_at = jnp.where(t == 0, 0, n_tp - 1)

    def slice_at(i):
        return lax.rem(t + i, n_tp)

    barrier = pltpu.get_barrier_semaphore()

    def greet(p):
        pl.semaphore_signal(barrier, inc=1, device_id={"ep": p}, device_id_type=MESH)

    pl.loop(e + 1, n_ep)(greet)

    @pl.when(mine == GROUPS - 1)
    def _():
        each(gs, greet)


    def greet_tp(p):
        pl.semaphore_signal(barrier, inc=1, device_id={"tp": p}, device_id_type=MESH)

    @pl.when(t == 0)
    def _():
        pl.loop(1, n_tp)(greet_tp)

    loads = [
        pltpu.make_async_copy(cho_hbm.at[e], cho, in_sem),
        pltpu.make_async_copy(wt_hbm.at[0], wt, in_sem),
        pltpu.make_async_copy(tok_hbm, tok, in_sem),
    ]
    for c in loads:
        c.start()
    wloads = []
    for i in range(n_tp):
        deep = pl.ds(pl.multiple_of(slice_at(i) * sw, sw), sw)
        col = pl.multiple_of(quarter_at(i) * sw, sw)
        wloads += [
            pltpu.make_async_copy(gate_hbm.at[0, deep, :], gate.at[deep, :], w_sem),
            pltpu.make_async_copy(up_hbm.at[0, deep, :], up.at[deep, :], w_sem),
            pltpu.make_async_copy(down_hbm.at[0, :, pl.ds(col, sw)], down.at[i], w_sem),
        ]

    with jax.named_scope("barrier"):
        floor = e + jnp.minimum(t, 1)

        @pl.when(mine > 0)
        def _():
            pl.semaphore_wait(barrier, floor)


    def answer(p):
        pl.semaphore_signal(ep_ready.at[e], inc=1, device_id={"ep": p}, device_id_type=MESH)

    @pl.when(mine > 0)
    def _():
        pl.loop(jnp.where(mine == GROUPS - 1, gs, 0), e)(answer)

    @pl.when(jnp.logical_and(t > 0, mine > 0))
    def _():
        pl.semaphore_signal(tp_seen, inc=1, device_id={"tp": 0}, device_id_type=MESH)

    with jax.named_scope("loadwait"):
        for c in loads:
            c.wait()
    for c in wloads:
        c.start()

    lane = lax.broadcasted_iota(jnp.int32, (picks, picks), 1)
    sub = lax.broadcasted_iota(jnp.int32, (picks, picks), 0)
    diag = lane == sub
    position = lax.broadcasted_iota(jnp.int32, (picks, tok_count), 1).astype(jnp.float32)
    columns, hots = [], []
    for x in range(experts):
        spread = jnp.broadcast_to(cho[x : x + 1, :], (picks, picks)).astype(jnp.float32)
        column = jnp.sum(jnp.where(diag, spread, 0.0), axis=1, keepdims=True)
        columns.append(column)
        hots.append(jnp.where(position == column, 1.0, 0.0))
    onehot = jnp.concatenate(hots, axis=0).astype(jnp.bfloat16)
    with jax.named_scope("gather"):
        for k in range(n_tp):
            sel = jnp.dot(
                onehot, tok[:, k * sw : (k + 1) * sw], preferred_element_type=jnp.float32
            )
            leaving[k] = sel.reshape(experts, picks, sw).astype(jnp.bfloat16)

    def send_tokens(k, p):
        return pltpu.make_async_remote_copy(
            src_ref=leaving.at[k, p],
            dst_ref=arrived.at[k, e],
            send_sem=s1_send,
            recv_sem=s1_recv.at[k],
            device_id={"ep": p},
            device_id_type=MESH,
        )

    def send_hop(slot, p):
        return pltpu.make_async_remote_copy(
            src_ref=leaving.at[t, p],
            dst_ref=arrived.at[t, e],
            send_sem=hop_send,
            recv_sem=hop_recv.at[slot],
            device_id={"ep": p},
            device_id_type=MESH,
        )

    odd = lax.rem(e, 2)

    def split_to(parity, dst):
        return any_of([mine == a for a, b in SPLIT[parity] if b == dst])

    def split_from(src):
        return any_of(
            jnp.logical_and(mine == b, odd == parity)
            for parity in range(2)
            for a, b in SPLIT[parity]
            if a == src
        )

    def hops_to(dst):
        for parity in range(2):
            for a, b in SPLIT[parity]:
                if b == dst:
                    @pl.when(mine == a)
                    def _():
                        each(gs // 2, lambda i: send_hop(a, b * gs + 2 * i + parity).start())

    def direct_to(dst):
        @pl.when(jnp.logical_not(split_to(1, dst)))
        def _():
            for i in range(n_tp):
                k = slice_at(i)
                each(gs, lambda j: send_tokens(k, dst * gs + j).start())

        @pl.when(jnp.logical_and(split_to(1, dst), jnp.logical_not(split_to(0, dst))))
        def _():
            for i in range(n_tp):
                k = slice_at(i)
                each(gs // 2, lambda j: send_tokens(k, dst * gs + 2 * j).start())

    def ready_group(g):
        each(gs, lambda i: pl.semaphore_wait(ep_ready.at[g * gs + i], 1))

    with jax.named_scope("senddown"):
        for dst in range(GROUPS - 2, -1, -1):
            @pl.when(mine > dst)
            def _():
                hops_to(dst)

        for dst in range(GROUPS - 1):
            @pl.when(mine > dst)
            def _():
                direct_to(dst)

        def send_near(i):
            p = mine * gs + i
            p = jnp.where(p < e, p, p + 1)

            @pl.when(p > e)
            def _():
                pl.semaphore_wait(ep_ready.at[p], 1)

            for k in range(n_tp):
                send_tokens(k, p).start()

        @pl.when(mine > 0)
        def _():
            each(gs - 1, send_near)

    with jax.named_scope("hop"):
        for dst in range(1, GROUPS):
            @pl.when(mine == dst - 1)
            def _():
                ready_group(dst)
                hops_to(dst)
                direct_to(dst)

    with jax.named_scope("tpseen"):
        def open_tp():
            pl.semaphore_wait(tp_seen, n_tp - 1)

            def admit(p):
                pl.semaphore_signal(tp_ready, inc=1, device_id={"tp": p}, device_id_type=MESH)

            pl.loop(1, n_tp)(admit)

        @pl.when(jnp.logical_and(t == 0, mine > 0))
        def _():
            open_tp()

    with jax.named_scope("sendup"):
        for dst in range(2, GROUPS):
            @pl.when(mine < dst - 1)
            def _():
                if dst < GROUPS - 1:
                    ready_group(dst)
                else:
                    @pl.when(mine == 0)
                    def _():
                        pl.semaphore_wait(barrier, floor + gs)

                    @pl.when(mine > 0)
                    def _():
                        ready_group(dst)

                hops_to(dst)
                direct_to(dst)

        @pl.when(mine == 0)
        def _():
            pl.loop(0, e)(answer)

            @pl.when(t > 0)
            def _():
                pl.semaphore_signal(tp_seen, inc=1, device_id={"tp": 0}, device_id_type=MESH)

            each(gs - 1, send_near)

            @pl.when(t == 0)
            def _():
                open_tp()


    parts = []
    for x in range(experts):
        wide = jnp.broadcast_to(wt[x : x + 1, :], (picks, picks))
        wcol = jnp.sum(jnp.where(diag, wide, 0.0), axis=1, keepdims=True)
        parts.append(jnp.where(position == columns[x], wcol, 0.0))
    weighted = jnp.concatenate(parts, axis=0)
    hi = weighted.astype(jnp.bfloat16).astype(jnp.float32)
    mid = weighted - hi
    place[...] = jnp.concatenate([hi, mid], axis=0).T.astype(jnp.bfloat16)

    def landed(ref, sem):
        pltpu.make_async_copy(ref, ref, sem).wait()


    @pl.when(t > 0)
    def _():
        pl.semaphore_wait(tp_ready, 1)

    @pl.when(mine == 0)
    def _():
        for i in range(n_tp - 1):
            pl.semaphore_signal(
                tp_above, inc=1, device_id={"tp": lax.rem(t + 1 + i, n_tp)}, device_id_type=MESH
            )

    def send_fan(slot, i):
        blocks = pl.ds(slot * gs, gs)
        return pltpu.make_async_remote_copy(
            src_ref=arrived.at[t, blocks],
            dst_ref=arrived.at[t, blocks],
            send_sem=fan_send,
            recv_sem=s1_recv.at[t],
            device_id={"tp": lax.rem(t + 1 + i, n_tp)},
            device_id_type=MESH,
        )

    with jax.named_scope("fan"):
        for slot in range(GROUPS):
            @pl.when(split_from(slot))
            def _():
                landed(arrived.at[t, pl.ds(0, gs)], hop_recv.at[slot])
                for i in range(n_tp - 1):
                    send_fan(slot, i).start()

    heard = {}
    for group in range(GROUPS):
        for parity in range(2):
            count = gs * sum(b == group for _, b in SPLIT[parity])
            case = jnp.logical_and(mine == group, odd == parity)
            heard[count] = jnp.logical_or(heard[count], case) if count in heard else case

    for k in range(n_tp):
        arrived[k, e] = leaving[k, e]
    @pl.when(mine == 0)
    def _():
        pl.semaphore_wait(tp_above, n_tp - 1)

    landed(gate, w_sem)
    landed(up, w_sem)
    landed(down, w_sem)
    hid = gate.shape[1]
    step = hid // COLUMNS
    hidden = []
    for i in range(n_tp):
        k = slice_at(i)
        with jax.named_scope(f'tokin#k={i}'):
            if i:
                landed(arrived.at[k, pl.ds(0, n_ep - 1)], s1_recv.at[k])
            else:
                for count in sorted(heard):
                    @pl.when(heard[count])
                    def _():
                        landed(arrived.at[k, pl.ds(0, n_ep - 1 - count)], s1_recv.at[k])

        x = arrived[k].astype(jnp.float32).reshape(rows, sw).astype(jnp.bfloat16)
        deep = pl.ds(pl.multiple_of(k * sw, sw), sw)
        for c in range(COLUMNS):
            cols = pl.ds(c * step, step)
            g = jnp.dot(x, gate[deep, cols], preferred_element_type=jnp.float32)
            u = jnp.dot(x, up[deep, cols], preferred_element_type=jnp.float32)
            if i > 0:
                g += gate_acc[:, cols]
                u += up_acc[:, cols]
            if i < n_tp - 1:
                gate_acc[:, cols] = g
                up_acc[:, cols] = u
            else:
                hidden.append((g / (1.0 + jnp.exp(-g)) * u).astype(jnp.bfloat16))

    def send_part(i, gi):
        blocks = pl.ds(group_at(gi) * gs, gs)
        return pltpu.make_async_remote_copy(
            src_ref=part_out.at[i, blocks],
            dst_ref=part_in.at[t, blocks],
            send_sem=s2_send,
            recv_sem=s2_recv.at[gi],
            device_id={"tp": quarter_at(i)},
            device_id_type=MESH,
        )

    def start_part(i, gi, when):
        @pl.when(jnp.logical_and(when, jnp.logical_not(direct(i, group_at(gi)))))
        def _():
            send_part(i, gi).start()

    def send_first(i, p):
        return pltpu.make_async_remote_copy(
            src_ref=part_out.at[i, p],
            dst_ref=first_in.at[t * n_ep + e],
            send_sem=first_send,
            recv_sem=first_recv,
            device_id={"ep": p, "tp": quarter_at(i)},
            device_id_type=MESH,
        )

    def start_first(i):
        for dst in (0, *range(GROUPS - 1, 0, -1)):
            @pl.when(direct(i, dst))
            def _():
                each(gs, lambda j: send_first(i, dst * gs + j).start())

    def send_back(p):
        return pltpu.make_async_remote_copy(
            src_ref=back_out.at[p],
            dst_ref=back_in.at[e],
            send_sem=s3_send,
            recv_sem=s3_recv,
            device_id={"ep": p},
            device_id_type=MESH,
        )

    for i in range(n_tp):
        with jax.named_scope(f'down#i={i}'):
            part = jnp.dot(hidden[0], down[i, pl.ds(0, step)], preferred_element_type=jnp.float32)
            for c in range(1, COLUMNS):
                part += jnp.dot(
                    hidden[c], down[i, pl.ds(c * step, step)], preferred_element_type=jnp.float32
                )
            part_out[i] = part.reshape(experts, picks, sw).astype(jnp.bfloat16)
        if i == 0:
            start_part(0, GROUPS - 1, jnp.logical_and(t > 0, mine == 0))
        start_first(i)
        here = leaves(i)
        if i < n_tp - 1:
            for gi in range(EARLY):
                start_part(i, gi, here)
            for gi in range(EARLY, GROUPS - 1):
                start_part(i, gi, here)
        else:
            for gi in range(GROUPS):
                start_part(i, gi, here)
        if i == n_tp - 2:
            for gi in range(EARLY, GROUPS):
                for x in range(n_tp - 1):
                    late = mine < 0 if gi < GROUPS - 1 else mine > (0 if x == 0 else -1)
                    start_part(x, gi, jnp.logical_and(leaves(x), late))

    for gi in range(GROUPS):
        gg = group_at(gi)

        ended = jnp.where(t == 0, direct(0, gg), direct(1, gg))

        @pl.when(jnp.logical_not(ended))
        def _():
            blocks = pl.ds(gg * gs, gs)
            total = part_out[own_at, blocks].astype(jnp.float32)
            with jax.named_scope(f'rs#g={gi}'):
                landed(part_in.at[pl.ds(0, n_tp - 1), blocks], s2_recv.at[gi])
            for i in range(n_tp - 1):
                total += part_in[lax.rem(t + 1 + i, n_tp), blocks].astype(jnp.float32)
            back_out[blocks] = total.astype(jnp.bfloat16)

            def give(i):
                p = gg * gs + i
                if gi < GROUPS - 1:
                    send_back(p).start()
                else:
                    @pl.when(p != e)
                    def _():
                        send_back(p).start()

            each(gs, give)

    back_in[e] = back_out[e]
    with jax.named_scope("drain"):
        for group in range(GROUPS):
            @pl.when(mine == group)
            def _():
                hops = gs // 2 * sum(a == group for pairs in SPLIT for a, _ in pairs)
                for k in range(n_tp):
                    landed(leaving.at[k, pl.ds(0, n_ep - 1 - hops)], s1_send)
                if hops:
                    landed(leaving.at[0, pl.ds(0, hops)], hop_send)

        for slot in range(GROUPS):
            @pl.when(split_from(slot))
            def _():
                landed(arrived.at[pl.ds(0, n_tp - 1), pl.ds(0, gs)], fan_send)

        def sent(lead, rest):
            firsts = gs * (lead + (n_tp - 1) * rest)
            if firsts:
                landed(first_in.at[pl.ds(0, firsts)], first_send)

            @pl.when(t == 0)
            def _():
                parts = (n_tp - 1) * (n_ep - gs * rest)
                landed(first_in.at[pl.ds(0, parts)], s2_send)
                landed(back_out.at[pl.ds(0, n_ep - 1 - gs * lead)], s3_send)

            @pl.when(t > 0)
            def _():
                parts = n_ep - gs * lead + (n_tp - 2) * (n_ep - gs * rest)
                landed(first_in.at[pl.ds(0, parts)], s2_send)
                landed(back_out.at[pl.ds(0, n_ep - 1 - gs * rest)], s3_send)

        for group in range(GROUPS):
            @pl.when(mine == group)
            def _():
                sent(sum(a == group for a, _ in FIRST), sum(a == group for a, _ in EVERY))

    ends = {}
    for group in range(GROUPS):
        for pairs, here in ((FIRST, t == 0), (EVERY, t > 0)):
            case = jnp.logical_and(mine == group, here)
            come = tuple(sorted(a for a, b in pairs if b == group))
            ends[come] = jnp.logical_or(ends[come], case) if come in ends else case

    for come in sorted(ends, key=len):
        @pl.when(ends[come])
        def _():
            with jax.named_scope('backin'):
                landed(back_in.at[pl.ds(0, n_ep - 1 - gs * len(come))], s3_recv)
            if come:
                with jax.named_scope('firstin'):
                    landed(first_in.at[pl.ds(0, n_tp * gs * len(come))], first_recv)
            for src in come:
                total = first_in[pl.ds(src * gs, gs)].astype(jnp.float32)
                for i in range(1, n_tp):
                    total += first_in[pl.ds(i * n_ep + src * gs, gs)].astype(jnp.float32)
                back_in[pl.ds(src * gs, gs)] = total.astype(jnp.bfloat16)

    with jax.named_scope("combine"):
        y = back_in[...].astype(jnp.float32).reshape(rows, sw).astype(jnp.bfloat16)
        y = jnp.concatenate([y, y], axis=0)
        result = jnp.dot(place[...], y, preferred_element_type=jnp.float32)
        out_ref[...] = result.astype(out_ref.dtype)


def local(tokens, chosen, chosen_weight, gate_weight, up_weight, down_weight):
    n_ep, n_tp = lax.axis_size("ep"), lax.axis_size("tp")
    tok_count, width = tokens.shape
    blocks, experts, picks = chosen.shape
    hid = gate_weight.shape[2]
    rows = blocks * picks
    sw = width // n_tp
    bf, f32 = jnp.bfloat16, jnp.float32
    dma = pltpu.SemaphoreType.DMA
    hbm = pl.BlockSpec(memory_space=pltpu.HBM)
    return pl.pallas_call(
        functools.partial(kernel, n_ep, n_tp),
        out_shape=jax.ShapeDtypeStruct((tok_count, sw), bf),
        in_specs=[hbm] * 6,
        out_specs=pl.BlockSpec(memory_space=pltpu.VMEM),
        scratch_shapes=[
            pltpu.VMEM((tok_count, width), bf),
            pltpu.VMEM((experts, picks), jnp.int32),
            pltpu.VMEM((experts, picks), f32),
            pltpu.VMEM((width, hid), bf),
            pltpu.VMEM((width, hid), bf),
            pltpu.VMEM((n_tp, hid, sw), bf),
            pltpu.VMEM((n_tp, experts, picks, sw), bf),
            pltpu.VMEM((n_tp, blocks, picks, sw), bf),
            pltpu.VMEM((rows, hid), f32),
            pltpu.VMEM((rows, hid), f32),
            pltpu.VMEM((tok_count, 2 * experts * picks), bf),
            pltpu.VMEM((n_tp, blocks, picks, sw), bf),
            pltpu.VMEM((n_tp, blocks, picks, sw), bf),
            pltpu.VMEM((n_tp * n_ep, picks, sw), bf),
            pltpu.VMEM((blocks, picks, sw), bf),
            pltpu.VMEM((experts, picks, sw), bf),
            dma,
            dma,
            dma,
            dma((n_tp,)),
            dma,
            dma((GROUPS,)),
            dma,
            dma,
            dma((GROUPS,)),
            dma,
            dma,
            dma,
            dma,
            pltpu.SemaphoreType.REGULAR((n_ep,)),
            pltpu.SemaphoreType.REGULAR,
            pltpu.SemaphoreType.REGULAR,
            pltpu.SemaphoreType.REGULAR,
        ],
        compiler_params=pltpu.CompilerParams(
            collective_id=0, has_side_effects=True, vmem_limit_bytes=32 * 1024 * 1024
        ),
    )(*(
        pltpu.with_memory_space_constraint(a, pltpu.HBM)
        for a in (tokens, chosen, chosen_weight, gate_weight, up_weight, down_weight)
    ))


def solution(mesh):
    return jax.shard_map(
        local,
        mesh=mesh,
        in_specs=(
            P("ep", None),
            P(),
            P("ep", None, None),
            P("ep", None, "tp"),
            P("ep", None, "tp"),
            P("ep", "tp", None),
        ),
        out_specs=P("ep", "tp"),
        check_vma=False,
    )
```
